512 devices in a mesh: sp: 32 (over z, core), tp: 16 (over y, x).
Axes of the slice: x: 4, y: 4, z: 16, core: 2. Of those that a mesh axis runs over, the one named last changes fastest.
Arguments:
- resid: bfloat16 [65536, 2048], P(('sp', 'tp')), may hold values from -6 to 6
- branch_input: bfloat16 [1024, 65536], P('tp', 'sp'), may hold values from -6 to 6
- gate_in: bfloat16 [1024, 65536], P('tp', 'sp'), may hold values from -6 to 6
- conv_taps: bfloat16 [4, 1024], P(None, 'tp'), may hold values from -3 to 3
- rate_weight: bfloat16 [16, 64, 64], P('tp'), may hold values from -0.75 to 0.75
- input_weight: bfloat16 [16, 64, 64], P('tp'), may hold values from -0.75 to 0.75
- decay_base: float32 [1024], P('tp')
- decay_extra: float32 [65536], P('sp'), may hold values from -2 to 0
- out_weight: bfloat16 [1024, 2048], P('tp'), may hold values from -0.1875 to 0.1875
- gain_mix: float32 [2048], replicated, may hold values from 0.1 to 1.9
- gain_pre: float32 [2048], replicated, may hold values from 0.1 to 1.9
- gain_post: float32 [2048], replicated, may hold values from 0.1 to 1.9
- expert_ids: int32 [65536, 2], P(('sp', 'tp')), may hold values from 0 to 31, as said below
- route_weight: float32 [65536, 2], P(('sp', 'tp')), may hold values from 0.2 to 1
- gate_proj: bfloat16 [32, 512, 2048], P('sp', 'tp'), may hold values from -0.125 to 0.125
- up_proj: bfloat16 [32, 512, 2048], P('sp', 'tp'), may hold values from -0.125 to 0.125
- down_proj: bfloat16 [32, 512, 2048], P('sp', 'tp'), may hold values from -0.25 to 0.25
Outputs:
- layer_out: bfloat16 [65536, 2048], P(('sp', 'tp'))
The draws below stay inside these ranges and needn't reach their ends.
Inputs may be any that keep to these rules, and one draw needn't show every extreme that they name: `expert_ids`: each row names two different experts of one group: both lie in g * 8 .. g * 8 + 7 for some g. In each aligned block of 128 rows (the rows of one device) every expert is named by exactly 8 rows.
All inputs are finite; a program needn't handle non-finite values.
Results may differ from the reference program's by a relative error of at most 0.0065.
Values may be sent and summed in bfloat16 or wider, within the bound.
A program may use at most 128 MiB of HBM per device.

```python
import math
import jax
import jax.numpy as jnp
from jax import lax

D = 2048
NB = 16
BLK = 64
R = 1024
CONV = 4
HID = 512
GROUPS = 4
TOP = 2
TOK_DEV = 128
EXPERTS = 32
EXP_GROUP = 8
TOK_SP = 2048
SEQUENCE_TOKENS = 65536


def draw_decay_base(key, part):
    random_subkeys = jax.random.split(key, 3)
    fast_share = 0.5
    picked = jax.random.uniform(random_subkeys[0], (R,), jnp.float32) < fast_share
    slow_rate = jnp.exp(jax.random.uniform(random_subkeys[1], (R,), jnp.float32, math.log(0.5), 0.0)) * (2.0 * math.log(2.0) / SEQUENCE_TOKENS)
    fast_rate = jnp.exp(jax.random.uniform(random_subkeys[2], (R,), jnp.float32, math.log(0.02), math.log(0.07)))
    step_rate = jnp.where(picked, fast_rate, slow_rate)
    return (-jnp.log(jnp.expm1(step_rate / 8.0))).astype(jnp.float32)


def draw_decay_extra(key, part):
    random_subkeys = jax.random.split(key, 3)
    blocks = SEQUENCE_TOKENS // TOK_SP
    factor = jnp.exp(jax.random.uniform(random_subkeys[0], (blocks,), jnp.float32, math.log(0.5), math.log(2.0)))
    baseline_value = -jnp.repeat(factor, TOK_SP, total_repeat_length=SEQUENCE_TOKENS) * (math.log(2.0) / SEQUENCE_TOKENS)
    spike_positions = jax.random.randint(random_subkeys[1], (2,), 0, SEQUENCE_TOKENS)
    spike_depth = jnp.log(jax.random.uniform(random_subkeys[2], (2,), jnp.float32, 0.6, 0.85))
    return baseline_value.at[spike_positions].add(spike_depth).astype(jnp.float32)


def draw_expert_ids(key, part):
    blocks = SEQUENCE_TOKENS // TOK_DEV
    per_group = TOK_DEV // GROUPS
    rank_list = jnp.arange(per_group, dtype=jnp.int32)
    lane_index = rank_list % EXP_GROUP
    round_index = rank_list // EXP_GROUP
    second = (lane_index + 1 + round_index % (EXP_GROUP - 1)) % EXP_GROUP
    first_lanes = jnp.tile(lane_index, GROUPS)
    second_lanes = jnp.tile(second, GROUPS)

    def member_perm(member_key):
        return jax.random.permutation(member_key, EXP_GROUP)

    def block_routes(block_key):
        random_subkeys = jax.random.split(block_key, 4)
        group_order = jax.random.permutation(random_subkeys[0], GROUPS)
        member_order = jax.vmap(member_perm)(jax.random.split(random_subkeys[1], GROUPS))
        slot_group = jnp.repeat(group_order, per_group, total_repeat_length=TOK_DEV)
        first_pick = slot_group * EXP_GROUP + member_order[slot_group, first_lanes]
        second_pick = slot_group * EXP_GROUP + member_order[slot_group, second_lanes]
        swapped = jax.random.randint(random_subkeys[2], (TOK_DEV,), 0, 2)
        paired = jnp.stack([jnp.where(swapped == 1, second_pick, first_pick), jnp.where(swapped == 1, first_pick, second_pick)], axis=1)
        row_order = jax.random.permutation(random_subkeys[3], TOK_DEV)
        return paired[row_order]
    routes = jax.vmap(block_routes)(jax.random.split(key, blocks))
    return routes.reshape(SEQUENCE_TOKENS, TOP).astype(jnp.int32)


def block_scale(own_key, dims, cuts, low, top_value):
    def one(axis_at, shards_of):
        steps = jax.random.uniform(jax.random.fold_in(jax.random.fold_in(own_key, 6), axis_at), (shards_of,), jnp.float32, low / len(cuts), top_value / len(cuts))
        return jnp.repeat(jnp.exp(steps), dims[axis_at] // shards_of).reshape((-1,) + (1,) * (len(dims) - axis_at - 1))

    level = one(*cuts[0])
    for cut in cuts[1:]:
        level = level * one(*cut)
    return level


def centred(stream_key, shape, spread, bound, cuts=(), kind=jnp.bfloat16):
    level = block_scale(stream_key, shape, cuts, -0.22, 0.18) if cuts else 1.0
    values = jax.random.normal(stream_key, shape, jnp.float32) * spread * level
    return jnp.minimum(jnp.maximum(values, -bound), bound).astype(kind)


def setup_inputs(seed: int = 0) -> dict:
    seeds = jax.random.split(jax.random.key(seed), 18)
    resid = centred(seeds[0], (SEQUENCE_TOKENS, D), 1.0, 6.0, ((0, 512),))
    branch_input = centred(seeds[1], (R, SEQUENCE_TOKENS), 1.0, 6.0, ((0, 16), (1, 32)))
    gate_in = centred(seeds[2], (R, SEQUENCE_TOKENS), 1.0, 6.0, ((0, 16), (1, 32)))
    conv_taps = centred(seeds[3], (CONV, R), CONV ** -0.5, 3.0, ((1, 16),))
    rate_weight = centred(seeds[4], (NB, BLK, BLK), BLK ** -0.5, 0.75, ((0, 16),))
    input_weight = centred(seeds[5], (NB, BLK, BLK), BLK ** -0.5, 0.75, ((0, 16),))
    decay_base = draw_decay_base(jax.random.fold_in(seeds[17], 71), 0)
    decay_extra = draw_decay_extra(jax.random.fold_in(seeds[17], 71), 0)
    out_weight = centred(seeds[8], (R, D), R ** -0.5, 0.1875, ((0, 16),))
    gain_mix = jnp.clip(1.0 + 0.18 * jax.random.normal(seeds[9], (D,), jnp.float32), 0.1, 1.9)
    gain_pre = jnp.clip(1.0 + 0.18 * jax.random.normal(seeds[10], (D,), jnp.float32), 0.1, 1.9)
    gain_post = jnp.clip(1.0 + 0.18 * jax.random.normal(seeds[11], (D,), jnp.float32), 0.1, 1.9)
    expert_ids = draw_expert_ids(jax.random.fold_in(seeds[17], 71), 0)
    route_weight = jnp.clip(0.2 + 0.8 * jax.random.uniform(seeds[13], (SEQUENCE_TOKENS, TOP), jnp.float32) ** block_scale(seeds[13], (SEQUENCE_TOKENS, TOP), ((0, 512),), -0.2, 0.2), 0.2, 1.0)
    gate_proj = centred(seeds[14], (EXPERTS, HID, D), D ** -0.5, 0.125, ((0, 32), (1, 16)))
    up_proj = centred(seeds[15], (EXPERTS, HID, D), D ** -0.5, 0.125, ((0, 32), (1, 16)))
    down_proj = centred(seeds[16], (EXPERTS, HID, D), HID ** -0.5, 0.25, ((0, 32), (1, 16)))
    return dict(resid=resid, branch_input=branch_input, gate_in=gate_in, conv_taps=conv_taps, rate_weight=rate_weight, input_weight=input_weight, decay_base=decay_base, decay_extra=decay_extra, out_weight=out_weight, gain_mix=gain_mix, gain_pre=gain_pre, gain_post=gain_post, expert_ids=expert_ids, route_weight=route_weight, gate_proj=gate_proj, up_proj=up_proj, down_proj=down_proj)


epsilon = 1e-06
gate_power = 8.0

def normalized(values, gain):
    return values * lax.rsqrt(lax.optimization_barrier(jnp.mean(values * values, axis=-1, keepdims=True)) + epsilon) * gain.astype(jnp.float32)

def combine_pair(earlier, latter):
    return (earlier[0] * latter[0], latter[0] * earlier[1] + latter[1])

def reference(resid, branch_input, gate_in, conv_taps, rate_weight, input_weight, decay_base, decay_extra, out_weight, gain_mix, gain_pre, gain_post, expert_ids, route_weight, gate_proj, up_proj, down_proj):
    blocks = SEQUENCE_TOKENS // TOK_SP
    branch_blocks = branch_input.reshape(R, blocks, TOK_SP).transpose(1, 0, 2)
    gate_blocks = gate_in.reshape(R, blocks, TOK_SP).transpose(1, 0, 2)
    extra_blocks = decay_extra.reshape(blocks, TOK_SP)
    resid_blocks = resid.reshape(blocks, TOK_SP, D)
    filter_tap_weights = conv_taps.astype(jnp.float32)
    decay_rate = -gate_power * jax.nn.softplus(-decay_base.astype(jnp.float32))
    decay_rate_matrix = rate_weight.astype(jnp.float32)
    input_matrix = input_weight.astype(jnp.float32)

    def advance(carried, pieces):
        edge_cols, entering = carried
        branch_block, gate_block, extra_block, resid_block = pieces
        padded = jnp.concatenate([edge_cols, branch_block.astype(jnp.float32)], axis=1)
        convolved = filter_tap_weights[0][:, None] * padded[:, 0:TOK_SP]
        for offset in range(1, CONV):
            convolved = convolved + filter_tap_weights[offset][:, None] * padded[:, offset:offset + TOK_SP]
        grouped = convolved.reshape(NB, BLK, TOK_SP)
        rate_gate = jax.nn.sigmoid(jnp.einsum('ncs,ncd->nds', grouped, decay_rate_matrix, precision=lax.Precision.HIGHEST).reshape(R, TOK_SP))
        input_gate = jax.nn.sigmoid(jnp.einsum('ncs,ncd->nds', grouped, input_matrix, precision=lax.Precision.HIGHEST).reshape(R, TOK_SP))
        log_keep = decay_rate[:, None] * rate_gate + extra_block[None, :]
        retain = jnp.exp(log_keep)
        driven = jnp.sqrt(-jnp.expm1(2.0 * log_keep)) * input_gate * convolved
        retained, local_state = lax.associative_scan(combine_pair, (retain, driven), axis=1)
        hidden_state = local_state + retained * entering[:, None]
        branch_out = (hidden_state * jax.nn.gelu(gate_block.astype(jnp.float32), approximate=True)).astype(jnp.bfloat16)
        mixed_rows = lax.dot_general(branch_out, out_weight, (((0,), (0,)), ((), ())), preferred_element_type=jnp.float32)
        after_mix = resid_block.astype(jnp.float32) + normalized(mixed_rows, gain_mix)
        ffn_in = normalized(after_mix, gain_pre).astype(jnp.bfloat16)
        return ((padded[:, TOK_SP:], hidden_state[:, -1]), (after_mix, ffn_in))
    start_state = (jnp.zeros((R, CONV - 1), jnp.float32), jnp.zeros((R,), jnp.float32))
    _, (after_mix, ffn_in) = lax.scan(advance, start_state, (branch_blocks, gate_blocks, extra_blocks, resid_blocks))
    after_mix = after_mix.reshape(SEQUENCE_TOKENS, D)
    ffn_in = ffn_in.reshape(SEQUENCE_TOKENS, D)
    chosen = expert_ids.reshape(-1).astype(jnp.int32)
    matches = (chosen[:, None] == jnp.arange(EXPERTS, dtype=jnp.int32)[None, :]).astype(jnp.int32)
    slot_index = lax.optimization_barrier(jnp.sum((jnp.cumsum(matches, axis=0) - 1) * matches, axis=1))
    per_expert = SEQUENCE_TOKENS * TOP // EXPERTS
    entries = jnp.zeros((EXPERTS * per_expert,), jnp.int32).at[chosen * per_expert + slot_index].set(jnp.arange(SEQUENCE_TOKENS * TOP, dtype=jnp.int32))
    entries = entries.reshape(EXPERTS, per_expert)
    weights_flat = route_weight.astype(jnp.float32).reshape(-1)

    def expert_step(totals, pieces):
        expert, entry_list = pieces
        token_index = entry_list // TOP
        picked_rows = ffn_in[token_index]
        gate_vals = jnp.dot(picked_rows, gate_proj[expert].T, preferred_element_type=jnp.float32)
        up_vals = jnp.dot(picked_rows, up_proj[expert].T, preferred_element_type=jnp.float32)
        hidden = (jax.nn.silu(gate_vals) * up_vals).astype(jnp.bfloat16)
        result = jnp.dot(hidden, down_proj[expert], preferred_element_type=jnp.float32).astype(jnp.bfloat16)
        weighted = result.astype(jnp.float32) * weights_flat[entry_list][:, None]
        return (totals.at[token_index].add(weighted), None)
    totals, _ = lax.scan(expert_step, jnp.zeros((SEQUENCE_TOKENS, D), jnp.float32), (jnp.arange(EXPERTS, dtype=jnp.int32), entries))
    return (after_mix + normalized(totals, gain_post)).astype(jnp.bfloat16)
```

```python
import functools
import math

import jax
import jax.numpy as jnp
from jax import lax
from jax.experimental import pallas as pl
from jax.experimental.pallas import tpu as pltpu
from jax.sharding import PartitionSpec as P

MESH = pl.DeviceIdType.MESH
F32 = jnp.float32
BF16 = jnp.bfloat16

epsilon = 1e-06
gate_power = 8.0
LANES = 128
COLS = 512
GROUP = 4


def one_minus_exp(y):
    series = F32(1.0 / 362880)
    for k in (40320, 5040, 720, 120, 24, 6, 2, 1):
        series = series * y + F32(1.0 / k)
    return jnp.where(y > -0.5, -y * series, 1.0 - jnp.exp(y))


def softplus(x):
    u = jnp.exp(-jnp.abs(x))
    series = F32(1.0 / 11)
    for k in range(10, 0, -1):
        series = F32(1.0 / k) - series * u
    return jnp.maximum(x, 0.0) + jnp.where(u < 0.125, u * series, jnp.log(1.0 + u))


def gelu(x):
    inner = F32(math.sqrt(2.0 / math.pi)) * (x + F32(0.044715) * (x * x * x))
    return x * (0.5 * (1.0 + jnp.tanh(inner)))


def to_column(row, size):
    lanes = row.shape[1]
    here = lax.broadcasted_iota(jnp.int32, (size, lanes), 0)
    there = lax.broadcasted_iota(jnp.int32, (size, lanes), 1)
    return jnp.sum(jnp.where(here == there, row, 0.0), axis=1, keepdims=True)


def kernel(
    cfg,
    resid_hbm,
    branch_ref,
    gate_ref,
    taps_ref,
    rate_w_ref,
    input_w_ref,
    base_ref,
    extra_ref,
    outw_hbm,
    gmix_ref,
    gpre_ref,
    gpost_ref,
    ids_ref,
    rw_ref,
    gp_hbm,
    up_hbm,
    dp_hbm,
    out_ref,
    resid_ref,
    keep_ref,
    state_ref,
    last_keep,
    last_state,
    act_ref,
    halo_ref,
    sum_ref,
    sums_ref,
    bo_ref,
    tok_ref,
    w_ref,
    e_ref,
    after_ref,
    ffn_ref,
    pick_ref,
    o_ref,
    x_ref,
    hid_ref,
    y_ref,
    r_ref,
    moe_ref,
    loc_sem,
    send_sem,
    recv_sem,
):
    nsp, nx, ny = cfg
    ntp = nx * ny
    sp = lax.axis_index("sp")
    tp = lax.axis_index("tp")
    my_x, my_y = lax.rem(tp, nx), lax.div(tp, nx)
    core = lax.rem(sp, 2)
    chan, positions = branch_ref.shape
    blocks = positions // LANES
    toks, width = resid_hbm.shape
    cap = o_ref.shape[1]
    slots = nsp * cap
    col_steps = width // COLS

    def remote(src, dst, k, to_sp, to_tp):
        return pltpu.make_async_remote_copy(
            src_ref=src, dst_ref=dst, send_sem=send_sem.at[k], recv_sem=recv_sem.at[k],
            device_id=(to_sp, to_tp), device_id_type=MESH,
        )

    def got(ref, k):
        pltpu.make_async_copy(ref, ref, recv_sem.at[k]).wait()

    def sent(ref, k):
        pltpu.make_async_copy(ref, ref, send_sem.at[k]).wait()

    own = [
        pltpu.make_async_copy(outw_hbm, w_ref.at[my_y, my_x], loc_sem.at[0]),
        pltpu.make_async_copy(gp_hbm, e_ref.at[0, my_y, my_x], loc_sem.at[1]),
        pltpu.make_async_copy(up_hbm, e_ref.at[1, my_y, my_x], loc_sem.at[2]),
        pltpu.make_async_copy(dp_hbm, e_ref.at[2, my_y, my_x], loc_sem.at[3]),
        pltpu.make_async_copy(resid_hbm, resid_ref, loc_sem.at[4]),
    ]
    for copy in own:
        copy.start()

    barrier = pltpu.get_barrier_semaphore()

    def greet_sp(k, carry):
        pl.semaphore_signal(
            barrier, inc=1, device_id=(lax.rem(sp + k, nsp), tp), device_id_type=MESH
        )
        return carry

    def greet_tp(k, carry):
        pl.semaphore_signal(
            barrier, inc=1, device_id=(sp, lax.rem(tp + k, ntp)), device_id_type=MESH
        )
        return carry

    lax.fori_loop(1, nsp, greet_sp, 0)
    lax.fori_loop(1, ntp, greet_tp, 0)

    taps = taps_ref[...].astype(F32)
    tap_cols = [to_column(taps[j : j + 1, :], chan) for j in range(4)]
    decay_rate = -gate_power * softplus(-to_column(base_ref[...], chan))
    lane = lax.broadcasted_iota(jnp.int32, (chan, LANES), 1)

    def lanes_of(index):
        return pl.ds(pl.multiple_of(index * LANES, LANES), LANES)

    def block_group(first, count, before):
        convs = []
        for g in range(count):
            cur = branch_ref[:, lanes_of(first + g)].astype(F32)
            total = tap_cols[3] * cur
            for back in (1, 2, 3):
                moved = jnp.where(
                    lane < back, pltpu.roll(before, back, 1), pltpu.roll(cur, back, 1)
                )
                total = total + tap_cols[3 - back] * moved
            convs.append(total)
            before = cur
        conv = jnp.concatenate(convs, axis=1)
        high = conv.astype(BF16)
        rest = conv - high.astype(F32)
        mid = rest.astype(BF16)
        low = (rest - mid.astype(F32)).astype(BF16)

        def gate_of(weight_ref):
            w = weight_ref[...]
            total = None
            for piece in (low, mid, high):
                part = lax.dot_general(
                    w, piece, (((0,), (0,)), ((), ())), preferred_element_type=F32
                )
                total = part if total is None else total + part
            return jax.nn.sigmoid(total)

        rate_gate = gate_of(rate_w_ref)
        input_gate = gate_of(input_w_ref)
        for g in range(count):
            at = slice(g * LANES, (g + 1) * LANES)
            extra = extra_ref[pl.ds(first + g, 1), :]
            log_keep = decay_rate * rate_gate[:, at] + extra
            keep = jnp.exp(log_keep)
            state = jnp.sqrt(one_minus_exp(2.0 * log_keep)) * input_gate[:, at] * convs[g]
            step = 1
            while step < LANES:
                inside = lane >= step
                keep_back = jnp.where(inside, pltpu.roll(keep, step, 1), 1.0)
                state_back = jnp.where(inside, pltpu.roll(state, step, 1), 0.0)
                state = keep * state_back + state
                keep = keep * keep_back
                step *= 2
            keep_ref[first + g] = keep
            state_ref[first + g] = state
            last_keep[first + g] = jnp.broadcast_to(keep[:, LANES - 1 :], (chan, LANES))
            last_state[first + g] = jnp.broadcast_to(state[:, LANES - 1 :], (chan, LANES))

    group = min(GROUP, blocks)

    def later_group(index, carry):
        first = index * group
        block_group(first, group, branch_ref[:, lanes_of(first - 1)].astype(F32))
        return carry

    lax.fori_loop(1, blocks // group, later_group, 0)

    pl.semaphore_wait(barrier, nsp - 1 + ntp - 1)
    remote(
        branch_ref.at[:, pl.ds(positions - LANES, LANES)], halo_ref, 0, lax.rem(sp + 1, nsp), tp
    ).start()

    own[0].wait()
    half_a, half_b = 2 * core, 2 * core + 1

    def tp_at(y, x):
        return lax.rem(y, ny) * nx + lax.rem(x, nx)

    for k in range(1, nx):
        ref = w_ref.at[my_y, my_x, half_a]
        remote(ref, ref, 1, sp, tp_at(my_y, my_x + k)).start()
    for k in range(1, ny):
        ref = w_ref.at[my_y, my_x, half_b]
        remote(ref, ref, 2, sp, tp_at(my_y + k, my_x)).start()

    got(halo_ref, 0)
    block_group(0, group, jnp.where(sp == 0, 0.0, halo_ref[...].astype(F32)))

    def chain(index, carry):
        keep, state = carry
        block_keep, block_state = last_keep[index], last_state[index]
        last_keep[index] = keep
        last_state[index] = state
        return (block_keep * keep, block_keep * state + block_state)

    all_keep, all_state = lax.fori_loop(
        0, blocks, chain, (jnp.ones((chan, LANES), F32), jnp.zeros((chan, LANES), F32))
    )
    row = lax.broadcasted_iota(jnp.int32, (chan, LANES), 0)
    summary = jnp.where(lane == row, all_keep, 0.0) + jnp.where(
        lane == row + chan, all_state, 0.0
    )
    sum_ref[...] = jnp.sum(summary, axis=0, keepdims=True)
    sums_ref[sp] = sum_ref[...]

    got(w_ref.at[0, pl.ds(0, nx - 1), 0], 1)
    for k in range(1, ny):
        ref = w_ref.at[my_y, :, half_a]
        remote(ref, ref, 3, sp, tp_at(my_y + k, my_x)).start()
    got(w_ref.at[pl.ds(0, ny - 1), 0, 0], 2)
    for k in range(1, nx):
        ref = w_ref.at[:, my_x, half_b]
        remote(ref, ref, 4, sp, tp_at(my_y, my_x + k)).start()

    def send_summary(k, carry):
        remote(sum_ref, sums_ref.at[sp], 5, lax.rem(sp + k, nsp), tp).start()
        return carry

    lax.fori_loop(1, nsp, send_summary, 0)

    def activate(index, carry):
        act_ref[index] = gelu(gate_ref[:, lanes_of(index)].astype(F32))
        return carry

    lax.fori_loop(0, blocks, activate, 0)

    ids = ids_ref[...]
    expert = lax.broadcasted_iota(jnp.int32, (nsp, toks), 0)
    named = [expert == ids[k : k + 1, :] for k in range(2)]
    counts = (named[0] | named[1]).astype(F32)
    token_a = lax.broadcasted_iota(jnp.int32, (toks, toks), 0)
    token_b = lax.broadcasted_iota(jnp.int32, (toks, toks), 1)
    earlier = jnp.dot(
        counts.astype(BF16), (token_a < token_b).astype(F32).astype(BF16),
        preferred_element_type=F32,
    )
    slot_at = [
        jnp.sum(
            jnp.where(named[k], earlier + (expert * cap).astype(F32), 0.0), axis=0, keepdims=True
        ).astype(jnp.int32)
        for k in range(2)
    ]
    slot = lax.broadcasted_iota(jnp.int32, (slots, toks), 0)
    chosen = [slot == slot_at[k] for k in range(2)]
    pick_ref[0] = (chosen[0] | chosen[1]).astype(F32).astype(BF16)
    weight = jnp.where(chosen[0], rw_ref[0:1, :], 0.0) + jnp.where(chosen[1], rw_ref[1:2, :], 0.0)
    weight_high = weight.astype(BF16)
    pick_ref[1] = weight_high
    pick_ref[2] = (weight - weight_high.astype(F32)).astype(BF16)

    got(sums_ref.at[pl.ds(0, nsp - 1)], 5)

    def fold(index, carry):
        line = sums_ref[index]
        keep = jnp.where(index < sp, to_column(line, chan), 1.0)
        moved = jnp.where(
            index < sp,
            jnp.sum(jnp.where(lane == row + chan, line, 0.0), axis=1, keepdims=True),
            0.0,
        )
        return keep * carry + moved

    entering = lax.fori_loop(0, nsp, fold, jnp.zeros((chan, 1), F32), unroll=True)

    def finish(index, carry):
        begin = last_state[index] + last_keep[index] * entering
        hidden = state_ref[index] + keep_ref[index] * begin
        bo_ref[index] = (hidden * act_ref[index]).astype(BF16)
        return carry

    lax.fori_loop(0, blocks, finish, 0)

    def send_tokens(k, carry):
        to = lax.rem(tp + k, ntp)
        remote(bo_ref.at[to], tok_ref.at[tp], 6, sp, to).start()
        return carry

    lax.fori_loop(1, ntp, send_tokens, 0)
    tok_ref[tp] = bo_ref[tp]

    got(w_ref.at[pl.ds(0, ny - 1), :, 0], 3)
    got(w_ref.at[:, pl.ds(0, nx - 1), 0], 4)
    ref = w_ref.at[:, :, pl.ds(2 * core, 2)]
    remote(ref, ref, 7, sp + 1 - 2 * core, tp).start()

    for copy in own[1:4]:
        copy.wait()
    for k in range(1, nx):
        ref = e_ref.at[:, my_y, my_x, 0]
        remote(ref, ref, 8, sp, tp_at(my_y, my_x + k)).start()
    for k in range(1, ny):
        ref = e_ref.at[:, my_y, my_x, 1]
        remote(ref, ref, 9, sp, tp_at(my_y + k, my_x)).start()

    own[4].wait()
    got(tok_ref.at[pl.ds(0, ntp - 1)], 6)
    got(w_ref.at[:, :, pl.ds(0, 2)], 7)

    def cols_of(index):
        return pl.ds(pl.multiple_of(index * COLS, COLS), COLS)

    def mix(index, carry):
        cols = cols_of(index)
        weights = w_ref[:, :, :, :, cols].reshape(ntp * chan, COLS)
        rows = tok_ref[...].reshape(ntp * chan, toks)
        after_ref[:, cols] = lax.dot_general(
            rows, weights, (((0,), (0,)), ((), ())), preferred_element_type=F32
        )
        return carry

    lax.fori_loop(0, col_steps, mix, 0)

    def scale(values):
        return lax.rsqrt(jnp.mean(values * values, axis=-1, keepdims=True) + epsilon)

    def rows_of(index):
        return pl.ds(pl.multiple_of(index * 16, 16), 16)

    def norms(index, carry):
        rows = rows_of(index)
        mixed = after_ref[rows, :]
        after = resid_ref[rows, :].astype(F32) + mixed * scale(mixed) * gmix_ref[...]
        after_ref[rows, :] = after
        ffn_ref[rows, :] = (after * scale(after) * gpre_ref[...]).astype(BF16)
        return carry

    lax.fori_loop(0, toks // 16, norms, 0)

    def spread(index, carry):
        cols = cols_of(index)
        o_ref[:, :, cols] = (
            jnp.dot(pick_ref[0], ffn_ref[:, cols], preferred_element_type=F32)
            .astype(BF16)
            .reshape(nsp, cap, COLS)
        )
        return carry

    lax.fori_loop(0, col_steps, spread, 0)

    def peer(k):
        away = lax.div(k + 1, 2)
        return lax.rem(lax.rem(k, 2) * away + (1 - lax.rem(k, 2)) * (nsp - away) + sp, nsp)

    def dispatch(k, carry):
        to = peer(k)
        remote(o_ref.at[to], x_ref.at[sp], 10, to, tp).start()
        return carry

    lax.fori_loop(1, nsp, dispatch, 0)
    x_ref[sp] = o_ref[sp]

    got(e_ref.at[:, 0, pl.ds(0, nx - 1), 0], 8)
    for k in range(1, ny):
        ref = e_ref.at[:, my_y, :, 0]
        remote(ref, ref, 11, sp, tp_at(my_y + k, my_x)).start()
    got(e_ref.at[:, pl.ds(0, ny - 1), 0, 1], 9)
    for k in range(1, nx):
        ref = e_ref.at[:, :, my_x, 1]
        remote(ref, ref, 12, sp, tp_at(my_y, my_x + k)).start()

    got(e_ref.at[:, pl.ds(0, ny - 1), :, 0], 11)
    got(e_ref.at[:, :, pl.ds(0, nx - 1), 1], 12)
    got(x_ref.at[pl.ds(0, nsp - 1)], 10)

    per_y = nx * 32
    nt = (((1,), (1,)), ((), ()))

    def expert_in(index, carry):
        ys = pl.ds(index * 2, 2)
        arriving = x_ref[...].reshape(slots, width)
        gate_rows = e_ref[0, ys].reshape(2 * per_y, width)
        up_rows = e_ref[1, ys].reshape(2 * per_y, width)
        gate_vals = lax.dot_general(arriving, gate_rows, nt, preferred_element_type=F32)
        up_vals = lax.dot_general(arriving, up_rows, nt, preferred_element_type=F32)
        hid_ref[index] = (gate_vals * jax.nn.sigmoid(gate_vals) * up_vals).astype(BF16)
        return carry

    lax.fori_loop(0, ny // 2, expert_in, 0)

    def expert_out(index, carry):
        cols = cols_of(index)
        total = None
        for half in range(ny // 2):
            down = e_ref[2, 2 * half : 2 * half + 2, :, :, :, cols].reshape(2 * per_y, COLS)
            part = jnp.dot(hid_ref[half], down, preferred_element_type=F32)
            total = part if total is None else total + part
        y_ref[:, :, cols] = total.astype(BF16).reshape(nsp, cap, COLS)
        return carry

    lax.fori_loop(0, col_steps, expert_out, 0)

    def give_back(k, carry):
        to = peer(k)
        remote(y_ref.at[to], r_ref.at[sp], 13, to, tp).start()
        return carry

    lax.fori_loop(1, nsp, give_back, 0)
    r_ref[sp] = y_ref[sp]
    got(r_ref.at[pl.ds(0, nsp - 1)], 13)

    def combine(index, carry):
        cols = cols_of(index)
        rows = r_ref[:, :, cols].reshape(slots, COLS)
        tn = (((0,), (0,)), ((), ()))
        moe_ref[:, cols] = lax.dot_general(
            pick_ref[2], rows, tn, preferred_element_type=F32
        ) + lax.dot_general(pick_ref[1], rows, tn, preferred_element_type=F32)
        return carry

    lax.fori_loop(0, col_steps, combine, 0)

    def finalize(index, carry):
        rows = rows_of(index)
        moe = moe_ref[rows, :]
        out_ref[rows, :] = (after_ref[rows, :] + moe * scale(moe) * gpost_ref[...]).astype(BF16)
        return carry

    lax.fori_loop(0, toks // 16, finalize, 0)

    sent(halo_ref, 0)
    sent(w_ref.at[0, pl.ds(0, nx - 1), 0], 1)
    sent(w_ref.at[pl.ds(0, ny - 1), 0, 0], 2)
    sent(w_ref.at[pl.ds(0, ny - 1), :, 0], 3)
    sent(w_ref.at[:, pl.ds(0, nx - 1), 0], 4)
    sent(sums_ref.at[pl.ds(0, nsp - 1)], 5)
    sent(tok_ref.at[pl.ds(0, ntp - 1)], 6)
    sent(w_ref.at[:, :, pl.ds(0, 2)], 7)
    sent(e_ref.at[:, 0, pl.ds(0, nx - 1), 0], 8)
    sent(e_ref.at[:, pl.ds(0, ny - 1), 0, 1], 9)
    sent(x_ref.at[pl.ds(0, nsp - 1)], 10)
    sent(e_ref.at[:, pl.ds(0, ny - 1), :, 0], 11)
    sent(e_ref.at[:, :, pl.ds(0, nx - 1), 1], 12)
    sent(r_ref.at[pl.ds(0, nsp - 1)], 13)


def solution(mesh):
    nsp, ntp = mesh.shape["sp"], mesh.shape["tp"]
    nx = math.isqrt(ntp)
    ny = ntp // nx

    def per_device(
        resid, branch_input, gate_in, conv_taps, rate_weight, input_weight, decay_base,
        decay_extra, out_weight, gain_mix, gain_pre, gain_post, expert_ids, route_weight,
        gate_proj, up_proj, down_proj,
    ):
        chan, positions = branch_input.shape
        toks, width = resid.shape
        blocks = positions // LANES
        cap = 2 * toks // nsp
        vmem = pl.BlockSpec(memory_space=pltpu.VMEM)
        hbm = pl.BlockSpec(memory_space=pl.ANY)
        block = (blocks, chan, LANES)
        return pl.pallas_call(
            functools.partial(kernel, (nsp, nx, ny)),
            out_shape=jax.ShapeDtypeStruct((toks, width), BF16),
            in_specs=[hbm] + [vmem] * 7 + [hbm] + [vmem] * 5 + [hbm] * 3,
            out_specs=vmem,
            scratch_shapes=[
                pltpu.VMEM((toks, width), BF16),
                pltpu.VMEM(block, F32),
                pltpu.VMEM(block, F32),
                pltpu.VMEM(block, F32),
                pltpu.VMEM(block, F32),
                pltpu.VMEM(block, F32),
                pltpu.VMEM((chan, LANES), BF16),
                pltpu.VMEM((1, LANES), F32),
                pltpu.VMEM((nsp, 1, LANES), F32),
                pltpu.VMEM(block, BF16),
                pltpu.VMEM((ntp, chan, toks), BF16),
                pltpu.VMEM((ny, nx, 4, chan // 4, width), BF16),
                pltpu.VMEM((3, ny, nx, 2, 16, width), BF16),
                pltpu.VMEM((toks, width), F32),
                pltpu.VMEM((toks, width), BF16),
                pltpu.VMEM((3, nsp * cap, toks), BF16),
                pltpu.VMEM((nsp, cap, width), BF16),
                pltpu.VMEM((nsp, cap, width), BF16),
                pltpu.VMEM((ny // 2, nsp * cap, nx * 64), BF16),
                pltpu.VMEM((nsp, cap, width), BF16),
                pltpu.VMEM((nsp, cap, width), BF16),
                pltpu.VMEM((toks, width), F32),
                pltpu.SemaphoreType.DMA((5,)),
                pltpu.SemaphoreType.DMA((14,)),
                pltpu.SemaphoreType.DMA((14,)),
            ],
            compiler_params=pltpu.CompilerParams(
                collective_id=0, has_side_effects=True, vmem_limit_bytes=52 * 1024 * 1024
            ),
        )(
            resid, branch_input, gate_in, conv_taps,
            rate_weight.reshape(chan, chan), input_weight.reshape(chan, chan),
            decay_base.reshape(1, chan), decay_extra.reshape(blocks, LANES),
            out_weight.reshape(4, chan // 4, width),
            gain_mix.reshape(1, width), gain_pre.reshape(1, width), gain_post.reshape(1, width),
            expert_ids.T, route_weight.T,
            gate_proj.reshape(2, 16, width), up_proj.reshape(2, 16, width),
            down_proj.reshape(2, 16, width),
        )

    sp_tp = P(("sp", "tp"), None)
    experts = P("sp", "tp", None)
    return jax.shard_map(
        per_device,
        mesh=mesh,
        in_specs=(
            sp_tp, P("tp", "sp"), P("tp", "sp"), P(None, "tp"),
            P("tp", None, None), P("tp", None, None), P("tp"), P("sp"), P("tp", None),
            P(), P(), P(), sp_tp, sp_tp, experts, experts, experts,
        ),
        out_specs=sp_tp,
        check_vma=False,
    )
```

```python
import functools
import math

import jax
import jax.numpy as jnp
from jax import lax
from jax.experimental import pallas as pl
from jax.experimental.pallas import tpu as pltpu
from jax.sharding import PartitionSpec as P

MESH = pl.DeviceIdType.MESH
F32 = jnp.float32
BF16 = jnp.bfloat16

epsilon = 1e-06
gate_power = 8.0
LANES = 128
COLS = 512
GROUP = 4
FAR = 22


def one_minus_exp(y):
    series = F32(1.0 / 362880)
    for k in (40320, 5040, 720, 120, 24, 6, 2, 1):
        series = series * y + F32(1.0 / k)
    return jnp.where(y > -0.5, -y * series, 1.0 - jnp.exp(y))


def softplus(x):
    u = jnp.exp(-jnp.abs(x))
    series = F32(1.0 / 11)
    for k in range(10, 0, -1):
        series = F32(1.0 / k) - series * u
    return jnp.maximum(x, 0.0) + jnp.where(u < 0.125, u * series, jnp.log(1.0 + u))


def gelu(x):
    inner = F32(math.sqrt(2.0 / math.pi)) * (x + F32(0.044715) * (x * x * x))
    return x * (0.5 * (1.0 + jnp.tanh(inner)))


def to_column(row, size):
    lanes = row.shape[1]
    here = lax.broadcasted_iota(jnp.int32, (size, lanes), 0)
    there = lax.broadcasted_iota(jnp.int32, (size, lanes), 1)
    return jnp.sum(jnp.where(here == there, row, 0.0), axis=1, keepdims=True)


def kernel(
    cfg,
    resid_hbm,
    branch_hbm,
    gate_hbm,
    taps_hbm,
    rate_w_hbm,
    input_w_hbm,
    base_hbm,
    extra_hbm,
    outw_hbm,
    gmix_hbm,
    gpre_hbm,
    gpost_hbm,
    ids_hbm,
    rw_hbm,
    gp_hbm,
    up_hbm,
    dp_hbm,
    out_ref,
    resid_ref,
    keep_ref,
    state_ref,
    last_keep,
    last_state,
    act_ref,
    halo_ref,
    sum_ref,
    sums_ref,
    bo_ref,
    tok_ref,
    w_ref,
    e_ref,
    after_ref,
    ffn_ref,
    pick_ref,
    o_ref,
    x_ref,
    on_ref,
    ob_ref,
    xb_ref,
    m_ref,
    xf_ref,
    hid_ref,
    y_ref,
    r_ref,
    moe_ref,
    branch_ref,
    gate_ref,
    taps_ref,
    rate_w_ref,
    input_w_ref,
    base_ref,
    extra_ref,
    gmix_ref,
    gpre_ref,
    gpost_ref,
    ids_ref,
    rw_ref,
    loc_sem,
    send_sem,
    recv_sem,
):
    nsp, nx, ny = cfg
    ntp = nx * ny
    sp = lax.axis_index("sp")
    tp = lax.axis_index("tp")
    my_x, my_y = lax.rem(tp, nx), lax.div(tp, nx)
    core = lax.rem(sp, 2)
    chan, positions = branch_hbm.shape
    blocks = positions // LANES
    toks, width = resid_hbm.shape
    cap = o_ref.shape[1]
    slots = nsp * cap
    col_steps = width // COLS

    def remote(src, dst, k, to_sp, to_tp):
        return pltpu.make_async_remote_copy(
            src_ref=src, dst_ref=dst, send_sem=send_sem.at[k], recv_sem=recv_sem.at[k],
            device_id=(to_sp, to_tp), device_id_type=MESH,
        )

    def got(ref, k):
        pltpu.make_async_copy(ref, ref, recv_sem.at[k]).wait()

    def sent(ref, k):
        pltpu.make_async_copy(ref, ref, send_sem.at[k]).wait()

    own = [
        pltpu.make_async_copy(outw_hbm, w_ref.at[my_y, my_x], loc_sem.at[0]),
        pltpu.make_async_copy(gp_hbm, e_ref.at[0, my_y, my_x], loc_sem.at[1]),
        pltpu.make_async_copy(up_hbm, e_ref.at[1, my_y, my_x], loc_sem.at[2]),
        pltpu.make_async_copy(dp_hbm, e_ref.at[2, my_y, my_x], loc_sem.at[3]),
        pltpu.make_async_copy(resid_hbm, resid_ref, loc_sem.at[4]),
    ]
    small = [
        pltpu.make_async_copy(source, target, loc_sem.at[5 + k])
        for k, (source, target) in enumerate((
            (branch_hbm, branch_ref), (taps_hbm, taps_ref), (rate_w_hbm, rate_w_ref),
            (input_w_hbm, input_w_ref), (base_hbm, base_ref), (extra_hbm, extra_ref),
            (gate_hbm, gate_ref), (ids_hbm, ids_ref), (rw_hbm, rw_ref),
            (gmix_hbm, gmix_ref), (gpre_hbm, gpre_ref), (gpost_hbm, gpost_ref),
        ))
    ]
    for copy in small + own:
        copy.start()

    barrier = pltpu.get_barrier_semaphore()

    def greet_sp(k, carry):
        pl.semaphore_signal(
            barrier, inc=1, device_id=(lax.rem(sp + k, nsp), tp), device_id_type=MESH
        )
        return carry

    def greet_tp(k, carry):
        pl.semaphore_signal(
            barrier, inc=1, device_id=(sp, lax.rem(tp + k, ntp)), device_id_type=MESH
        )
        return carry

    lax.fori_loop(1, nsp, greet_sp, 0)
    lax.fori_loop(1, ntp, greet_tp, 0)

    for copy in small[:6]:
        copy.wait()

    taps = taps_ref[...].astype(F32)
    tap_cols = [to_column(taps[j : j + 1, :], chan) for j in range(4)]
    decay_rate = -gate_power * softplus(-to_column(base_ref[...], chan))
    lane = lax.broadcasted_iota(jnp.int32, (chan, LANES), 1)

    def lanes_of(index):
        return pl.ds(pl.multiple_of(index * LANES, LANES), LANES)

    def block_group(first, count, before):
        convs = []
        for g in range(count):
            cur = branch_ref[:, lanes_of(first + g)].astype(F32)
            total = tap_cols[3] * cur
            for back in (1, 2, 3):
                moved = jnp.where(
                    lane < back, pltpu.roll(before, back, 1), pltpu.roll(cur, back, 1)
                )
                total = total + tap_cols[3 - back] * moved
            convs.append(total)
            before = cur
        conv = jnp.concatenate(convs, axis=1)
        high = conv.astype(BF16)
        rest = conv - high.astype(F32)
        mid = rest.astype(BF16)
        low = (rest - mid.astype(F32)).astype(BF16)

        def gate_of(weight_ref):
            w = weight_ref[...]
            total = None
            for piece in (low, mid, high):
                part = lax.dot_general(
                    w, piece, (((0,), (0,)), ((), ())), preferred_element_type=F32
                )
                total = part if total is None else total + part
            return jax.nn.sigmoid(total)

        rate_gate = gate_of(rate_w_ref)
        input_gate = gate_of(input_w_ref)
        for g in range(count):
            at = slice(g * LANES, (g + 1) * LANES)
            extra = extra_ref[pl.ds(first + g, 1), :]
            log_keep = decay_rate * rate_gate[:, at] + extra
            keep = jnp.exp(log_keep)
            state = jnp.sqrt(one_minus_exp(2.0 * log_keep)) * input_gate[:, at] * convs[g]
            step = 1
            while step < LANES:
                inside = lane >= step
                keep_back = jnp.where(inside, pltpu.roll(keep, step, 1), 1.0)
                state_back = jnp.where(inside, pltpu.roll(state, step, 1), 0.0)
                state = keep * state_back + state
                keep = keep * keep_back
                step *= 2
            keep_ref[first + g] = keep
            state_ref[first + g] = state
            last_keep[first + g] = jnp.broadcast_to(keep[:, LANES - 1 :], (chan, LANES))
            last_state[first + g] = jnp.broadcast_to(state[:, LANES - 1 :], (chan, LANES))

    group = min(GROUP, blocks)

    def later_group(index, carry):
        first = index * group
        block_group(first, group, branch_ref[:, lanes_of(first - 1)].astype(F32))
        return carry

    lax.fori_loop(1, blocks // group, later_group, 0)

    for copy in small[6:]:
        copy.wait()

    def activate(index, carry):
        act_ref[index] = gelu(gate_ref[:, lanes_of(index)].astype(F32))
        return carry

    lax.fori_loop(0, blocks, activate, 0)

    ids = ids_ref[...]
    expert = lax.broadcasted_iota(jnp.int32, (nsp, toks), 0)
    named = [expert == ids[k : k + 1, :] for k in range(2)]
    counts = (named[0] | named[1]).astype(F32)
    token_a = lax.broadcasted_iota(jnp.int32, (toks, toks), 0)
    token_b = lax.broadcasted_iota(jnp.int32, (toks, toks), 1)
    earlier = jnp.dot(
        counts.astype(BF16), (token_a < token_b).astype(F32).astype(BF16),
        preferred_element_type=F32,
    )
    slot_at = [
        jnp.sum(
            jnp.where(named[k], earlier + (expert * cap).astype(F32), 0.0), axis=0, keepdims=True
        ).astype(jnp.int32)
        for k in range(2)
    ]
    slot = lax.broadcasted_iota(jnp.int32, (slots, toks), 0)
    chosen = [slot == slot_at[k] for k in range(2)]
    pick_ref[0] = (chosen[0] | chosen[1]).astype(F32).astype(BF16)
    weight = jnp.where(chosen[0], rw_ref[0:1, :], 0.0) + jnp.where(chosen[1], rw_ref[1:2, :], 0.0)
    weight_high = weight.astype(BF16)
    pick_ref[1] = weight_high
    pick_ref[2] = (weight - weight_high.astype(F32)).astype(BF16)

    own[4].wait()

    def cols_of(index):
        return pl.ds(pl.multiple_of(index * COLS, COLS), COLS)

    def spread(rows_ref, slots_ref):
        def some(index, carry):
            cols = cols_of(index)
            slots_ref[:, :, cols] = (
                jnp.dot(pick_ref[0], rows_ref[:, cols], preferred_element_type=F32)
                .astype(BF16)
                .reshape(nsp, cap, COLS)
            )
            return carry

        lax.fori_loop(0, col_steps, some, 0)

    spread(resid_ref, o_ref)

    far = nsp * FAR // 32

    def peer(k):
        away = lax.div(k + 1, 2)
        return lax.rem(lax.rem(k, 2) * away + (1 - lax.rem(k, 2)) * (nsp - away) + sp, nsp)

    def send_block(source, target, sem, k, place):
        to = peer(k)
        remote(source.at[to], target.at[place], sem, to, tp).start()

    def send_blocks(source, target, sem, begin, end, offset=0):
        def step(k, carry):
            send_block(source, target, sem, k, k + 2 * lax.rem(k, 2) - 1 - offset)
            return carry

        lax.fori_loop(begin, end, step, 0)

    first_batch = min(far + 2, nsp - 1)

    pl.semaphore_wait(barrier, nsp - 1 + ntp - 1)
    remote(
        branch_ref.at[:, pl.ds(positions - LANES, LANES)], halo_ref, 0, lax.rem(sp + 1, nsp), tp
    ).start()

    send_block(o_ref, x_ref, 14, far - 1, far)
    send_blocks(o_ref, x_ref, 14, far + 1, first_batch)

    own[0].wait()
    half_a, half_b = 2 * core, 2 * core + 1

    def tp_at(y, x):
        return lax.rem(y, ny) * nx + lax.rem(x, nx)

    for k in range(1, nx):
        ref = w_ref.at[my_y, my_x, half_a]
        remote(ref, ref, 1, sp, tp_at(my_y, my_x + k)).start()
    for k in range(1, ny):
        ref = w_ref.at[my_y, my_x, half_b]
        remote(ref, ref, 2, sp, tp_at(my_y + k, my_x)).start()

    for copy in own[1:4]:
        copy.wait()
    for k in range(1, nx):
        ref = e_ref.at[:, my_y, my_x, 0]
        remote(ref, ref, 8, sp, tp_at(my_y, my_x + k)).start()
    for k in range(1, ny):
        ref = e_ref.at[:, my_y, my_x, 1]
        remote(ref, ref, 9, sp, tp_at(my_y + k, my_x)).start()

    got(halo_ref, 0)
    block_group(0, group, jnp.where(sp == 0, 0.0, halo_ref[...].astype(F32)))

    def chain(index, carry):
        keep, state = carry
        block_keep, block_state = last_keep[index], last_state[index]
        last_keep[index] = keep
        last_state[index] = state
        return (block_keep * keep, block_keep * state + block_state)

    all_keep, all_state = lax.fori_loop(
        0, blocks, chain, (jnp.ones((chan, LANES), F32), jnp.zeros((chan, LANES), F32))
    )
    row = lax.broadcasted_iota(jnp.int32, (chan, LANES), 0)
    summary = jnp.where(lane == row, all_keep, 0.0) + jnp.where(
        lane == row + chan, all_state, 0.0
    )
    sum_ref[...] = jnp.sum(summary, axis=0, keepdims=True)
    sums_ref[sp] = sum_ref[...]

    def send_summary(k, carry):
        remote(sum_ref, sums_ref.at[sp], 5, lax.rem(sp + k, nsp), tp).start()
        return carry

    lax.fori_loop(1, nsp, send_summary, 0)
    send_blocks(o_ref, x_ref, 14, first_batch, nsp - 1)
    send_block(o_ref, x_ref, 14, nsp - 1, nsp - 1)

    got(sums_ref.at[pl.ds(0, nsp - 1)], 5)

    def fold(index, carry):
        line = sums_ref[index]
        keep = jnp.where(index < sp, to_column(line, chan), 1.0)
        moved = jnp.where(
            index < sp,
            jnp.sum(jnp.where(lane == row + chan, line, 0.0), axis=1, keepdims=True),
            0.0,
        )
        return keep * carry + moved

    entering = lax.fori_loop(0, nsp, fold, jnp.zeros((chan, 1), F32), unroll=True)

    def finish(index, carry):
        begin = last_state[index] + last_keep[index] * entering
        hidden = state_ref[index] + keep_ref[index] * begin
        bo_ref[index] = (hidden * act_ref[index]).astype(BF16)
        return carry

    lax.fori_loop(0, blocks, finish, 0)

    def send_tokens(k, carry):
        to = lax.rem(tp + k, ntp)
        remote(bo_ref.at[to], tok_ref.at[tp], 6, sp, to).start()
        return carry

    lax.fori_loop(1, ntp, send_tokens, 0)
    tok_ref[tp] = bo_ref[tp]

    got(w_ref.at[0, pl.ds(0, nx - 1), 0], 1)
    for k in range(1, ny):
        ref = w_ref.at[my_y, :, half_a]
        remote(ref, ref, 3, sp, tp_at(my_y + k, my_x)).start()
    got(w_ref.at[pl.ds(0, ny - 1), 0, 0], 2)
    for k in range(1, nx):
        ref = w_ref.at[:, my_x, half_b]
        remote(ref, ref, 4, sp, tp_at(my_y, my_x + k)).start()

    got(e_ref.at[:, 0, pl.ds(0, nx - 1), 0], 8)
    for k in sorted({1, ny - 1}):
        ref = e_ref.at[:, my_y, :, 0]
        remote(ref, ref, 11, sp, tp_at(my_y + k, my_x)).start()
    got(e_ref.at[:, pl.ds(0, ny - 1), 0, 1], 9)
    for k in sorted({1, nx - 1}):
        ref = e_ref.at[:, :, my_x, 1]
        remote(ref, ref, 12, sp, tp_at(my_y, my_x + k)).start()

    got(tok_ref.at[pl.ds(0, ntp - 1)], 6)
    ob_ref[...] = (
        lax.dot_general(
            pick_ref[0], tok_ref[...].reshape(ntp * chan, toks), (((1,), (1,)), ((), ())),
            preferred_element_type=F32,
        )
        .astype(BF16)
        .reshape(nsp, cap, ntp * chan)
    )
    send_block(ob_ref, xb_ref, 15, far - 1, 0)
    send_blocks(ob_ref, xb_ref, 15, far + 1, nsp - 1, far)
    send_block(ob_ref, xb_ref, 15, nsp - 1, nsp - 1 - far)

    got(w_ref.at[pl.ds(0, ny - 1), :, 0], 3)
    got(w_ref.at[:, pl.ds(0, nx - 1), 0], 4)
    ref = w_ref.at[:, :, pl.ds(2 * core, 2)]
    remote(ref, ref, 7, sp + 1 - 2 * core, tp).start()
    got(w_ref.at[:, :, pl.ds(0, 2)], 7)

    def scale(values):
        return lax.rsqrt(jnp.mean(values * values, axis=-1, keepdims=True) + epsilon)

    def rows_of(index):
        return pl.ds(pl.multiple_of(index * 16, 16), 16)

    def projection(cols):
        return w_ref[:, :, :, :, cols].reshape(ntp * chan, COLS)

    def mix(index, carry):
        cols = cols_of(index)
        rows = tok_ref[...].reshape(ntp * chan, toks)
        moe_ref[:, cols] = lax.dot_general(
            rows, projection(cols), (((0,), (0,)), ((), ())), preferred_element_type=F32
        )
        return carry

    lax.fori_loop(0, col_steps, mix, 0)

    def norms(index, carry):
        rows = rows_of(index)
        mixed = moe_ref[rows, :]
        after = resid_ref[rows, :].astype(F32) + mixed * scale(mixed) * gmix_ref[...]
        after_ref[rows, :] = after
        ffn_ref[rows, :] = (after * scale(after) * gpre_ref[...]).astype(BF16)
        return carry

    lax.fori_loop(0, toks // 16, norms, 0)

    spread(ffn_ref, on_ref)
    send_blocks(on_ref, x_ref, 10, 1, far - 1)
    send_block(on_ref, x_ref, 10, far, far - 1)
    x_ref[0] = on_ref[sp]

    got(e_ref.at[:, pl.ds(0, min(2, ny - 1)), :, 0], 11)
    if ny > 2:
        before, after = lax.rem(my_y + ny - 1, ny), lax.rem(my_y + 1, ny)
        ref = e_ref.at[:, before, :, 0, :, pl.ds(0, width // 2)]
        remote(ref, ref, 16, sp, tp_at(after, my_x)).start()
        ref = e_ref.at[:, after, :, 0, :, pl.ds(width // 2, width // 2)]
        remote(ref, ref, 16, sp, tp_at(before, my_x)).start()
    got(e_ref.at[:, :, pl.ds(0, min(2, nx - 1)), 1], 12)
    if nx > 2:
        before, after = lax.rem(my_x + nx - 1, nx), lax.rem(my_x + 1, nx)
        ref = e_ref.at[:, :, before, 1, :, pl.ds(0, width // 2)]
        remote(ref, ref, 17, sp, tp_at(my_y, after)).start()
        ref = e_ref.at[:, :, after, 1, :, pl.ds(width // 2, width // 2)]
        remote(ref, ref, 17, sp, tp_at(my_y, before)).start()
    if ny > 2:
        got(e_ref.at[:, 0, :, 0], 16)
    if nx > 2:
        got(e_ref.at[:, :, 0, 1], 17)

    per_y = nx * 32
    nt = (((1,), (1,)), ((), ()))
    sources = max(16 // cap, 1)

    def rows_at(index):
        count = sources * cap
        return pl.ds(pl.multiple_of(index * count, count), count)

    def blocks_at(base, index):
        return x_ref[pl.ds(base + index * sources, sources)].reshape(sources * cap, width)

    def serve(base, end):
        rows = (end - base) * cap

        def expert_in(index, carry):
            ys = pl.ds(index * 2, 2)
            gate_rows = e_ref[0, ys].reshape(2 * per_y, width)
            up_rows = e_ref[1, ys].reshape(2 * per_y, width)
            inputs = xf_ref[0:rows, :]
            gate_vals = lax.dot_general(inputs, gate_rows, nt, preferred_element_type=F32)
            up_vals = lax.dot_general(inputs, up_rows, nt, preferred_element_type=F32)
            hid_ref[index, 0:rows, :] = (
                gate_vals * jax.nn.sigmoid(gate_vals) * up_vals
            ).astype(BF16)
            return carry

        lax.fori_loop(0, ny // 2, expert_in, 0)

        def expert_out(index, carry):
            cols = cols_of(index)
            total = None
            for pair in range(ny // 2):
                down = e_ref[2, 2 * pair : 2 * pair + 2, :, :, :, cols].reshape(2 * per_y, COLS)
                product = jnp.dot(hid_ref[pair, 0:rows, :], down, preferred_element_type=F32)
                total = product if total is None else total + product
            y_ref[base:end, :, cols] = total.astype(BF16).reshape(end - base, cap, COLS)
            return carry

        lax.fori_loop(0, col_steps, expert_out, 0)

        def give_back(k, carry):
            remote(y_ref.at[k], r_ref.at[sp], 13, peer(k), tp).start()
            return carry

        lax.fori_loop(max(base, 1), end, give_back, 0)

    got(x_ref.at[pl.ds(0, nsp - far)], 14)
    got(xb_ref, 15)

    def mix_arrived(index, carry):
        cols = cols_of(index)
        m_ref[:, cols] = jnp.dot(
            xb_ref[...].reshape((nsp - far) * cap, ntp * chan), projection(cols),
            preferred_element_type=F32,
        )
        return carry

    lax.fori_loop(0, col_steps, mix_arrived, 0)

    def norm_arrived(index, carry):
        rows = rows_at(index)
        mixed = m_ref[rows, :]
        after = (
            blocks_at(far, index).astype(F32) + mixed * scale(mixed) * gmix_ref[...]
        )
        xf_ref[rows, :] = (after * scale(after) * gpre_ref[...]).astype(BF16)
        return carry

    lax.fori_loop(0, (nsp - far) // sources, norm_arrived, 0)
    serve(far, nsp)

    got(x_ref.at[pl.ds(0, far - 1)], 10)

    def take_arrived(index, carry):
        xf_ref[rows_at(index), :] = blocks_at(0, index)
        return carry

    lax.fori_loop(0, far // sources, take_arrived, 0)
    serve(0, far)
    r_ref[sp] = y_ref[0]
    got(r_ref.at[pl.ds(0, nsp - 1)], 13)

    def combine(index, carry):
        cols = cols_of(index)
        rows = r_ref[:, :, cols].reshape(slots, COLS)
        tn = (((0,), (0,)), ((), ()))
        moe_ref[:, cols] = lax.dot_general(
            pick_ref[2], rows, tn, preferred_element_type=F32
        ) + lax.dot_general(pick_ref[1], rows, tn, preferred_element_type=F32)
        return carry

    lax.fori_loop(0, col_steps, combine, 0)

    def finalize(index, carry):
        rows = rows_of(index)
        moe = moe_ref[rows, :]
        out_ref[rows, :] = (after_ref[rows, :] + moe * scale(moe) * gpost_ref[...]).astype(BF16)
        return carry

    lax.fori_loop(0, toks // 16, finalize, 0)

    sent(halo_ref, 0)
    sent(w_ref.at[0, pl.ds(0, nx - 1), 0], 1)
    sent(w_ref.at[pl.ds(0, ny - 1), 0, 0], 2)
    sent(w_ref.at[pl.ds(0, ny - 1), :, 0], 3)
    sent(w_ref.at[:, pl.ds(0, nx - 1), 0], 4)
    sent(sums_ref.at[pl.ds(0, nsp - 1)], 5)
    sent(tok_ref.at[pl.ds(0, ntp - 1)], 6)
    sent(w_ref.at[:, :, pl.ds(0, 2)], 7)
    sent(e_ref.at[:, 0, pl.ds(0, nx - 1), 0], 8)
    sent(e_ref.at[:, pl.ds(0, ny - 1), 0, 1], 9)
    sent(x_ref.at[pl.ds(0, far - 1)], 10)
    sent(x_ref.at[pl.ds(0, nsp - far)], 14)
    sent(xb_ref, 15)
    sent(e_ref.at[:, pl.ds(0, min(2, ny - 1)), :, 0], 11)
    if ny > 2:
        sent(e_ref.at[:, 0, :, 0], 16)
    sent(e_ref.at[:, :, pl.ds(0, min(2, nx - 1)), 1], 12)
    if nx > 2:
        sent(e_ref.at[:, :, 0, 1], 17)
    sent(r_ref.at[pl.ds(0, nsp - 1)], 13)


def solution(mesh):
    nsp, ntp = mesh.shape["sp"], mesh.shape["tp"]
    nx = math.isqrt(ntp)
    ny = ntp // nx

    def per_device(
        resid, branch_input, gate_in, conv_taps, rate_weight, input_weight, decay_base,
        decay_extra, out_weight, gain_mix, gain_pre, gain_post, expert_ids, route_weight,
        gate_proj, up_proj, down_proj,
    ):
        chan, positions = branch_input.shape
        toks, width = resid.shape
        blocks = positions // LANES
        cap = 2 * toks // nsp
        vmem = pl.BlockSpec(memory_space=pltpu.VMEM)
        hbm = pl.BlockSpec(memory_space=pltpu.HBM)
        block = (blocks, chan, LANES)
        far = nsp * FAR // 32
        return pl.pallas_call(
            functools.partial(kernel, (nsp, nx, ny)),
            out_shape=jax.ShapeDtypeStruct((toks, width), BF16),
            in_specs=[hbm] * 17,
            out_specs=vmem,
            scratch_shapes=[
                pltpu.VMEM((toks, width), BF16),
                pltpu.VMEM(block, F32),
                pltpu.VMEM(block, F32),
                pltpu.VMEM(block, F32),
                pltpu.VMEM(block, F32),
                pltpu.VMEM(block, F32),
                pltpu.VMEM((chan, LANES), BF16),
                pltpu.VMEM((1, LANES), F32),
                pltpu.VMEM((nsp, 1, LANES), F32),
                pltpu.VMEM(block, BF16),
                pltpu.VMEM((ntp, chan, toks), BF16),
                pltpu.VMEM((ny, nx, 4, chan // 4, width), BF16),
                pltpu.VMEM((3, ny, nx, 2, 16, width), BF16),
                pltpu.VMEM((toks, width), F32),
                pltpu.VMEM((toks, width), BF16),
                pltpu.VMEM((3, nsp * cap, toks), BF16),
                pltpu.VMEM((nsp, cap, width), BF16),
                pltpu.VMEM((nsp, cap, width), BF16),
                pltpu.VMEM((nsp, cap, width), BF16),
                pltpu.VMEM((nsp, cap, ntp * chan), BF16),
                pltpu.VMEM((nsp - far, cap, ntp * chan), BF16),
                pltpu.VMEM(((nsp - far) * cap, width), F32),
                pltpu.VMEM((max(far, nsp - far) * cap, width), BF16),
                pltpu.VMEM((ny // 2, max(far, nsp - far) * cap, nx * 64), BF16),
                pltpu.VMEM((nsp, cap, width), BF16),
                pltpu.VMEM((nsp, cap, width), BF16),
                pltpu.VMEM((toks, width), F32),
                pltpu.VMEM((chan, positions), BF16),
                pltpu.VMEM((chan, positions), BF16),
                pltpu.VMEM(conv_taps.shape, BF16),
                pltpu.VMEM((chan, chan), BF16),
                pltpu.VMEM((chan, chan), BF16),
                pltpu.VMEM((1, chan), F32),
                pltpu.VMEM((blocks, LANES), F32),
                pltpu.VMEM((1, width), F32),
                pltpu.VMEM((1, width), F32),
                pltpu.VMEM((1, width), F32),
                pltpu.VMEM((2, toks), jnp.int32),
                pltpu.VMEM((2, toks), F32),
                pltpu.SemaphoreType.DMA((17,)),
                pltpu.SemaphoreType.DMA((18,)),
                pltpu.SemaphoreType.DMA((18,)),
            ],
            compiler_params=pltpu.CompilerParams(
                collective_id=0, has_side_effects=True, vmem_limit_bytes=67043328
            ),
        )(
            resid, branch_input, gate_in, conv_taps,
            rate_weight.reshape(chan, chan), input_weight.reshape(chan, chan),
            decay_base.reshape(1, chan), decay_extra.reshape(blocks, LANES),
            out_weight.reshape(4, chan // 4, width),
            gain_mix.reshape(1, width), gain_pre.reshape(1, width), gain_post.reshape(1, width),
            expert_ids.T, route_weight.T,
            gate_proj.reshape(2, 16, width), up_proj.reshape(2, 16, width),
            down_proj.reshape(2, 16, width),
        )

    sp_tp = P(("sp", "tp"), None)
    experts = P("sp", "tp", None)
    return jax.shard_map(
        per_device,
        mesh=mesh,
        in_specs=(
            sp_tp, P("tp", "sp"), P("tp", "sp"), P(None, "tp"),
            P("tp", None, None), P("tp", None, None), P("tp"), P("sp"), P("tp", None),
            P(), P(), P(), sp_tp, sp_tp, experts, experts, experts,
        ),
        out_specs=sp_tp,
        check_vma=False,
    )
```

```python
import functools
import math

import jax
import jax.numpy as jnp
from jax import lax
from jax.experimental import pallas as pl
from jax.experimental.pallas import tpu as pltpu
from jax.sharding import PartitionSpec as P

MESH = pl.DeviceIdType.MESH
F32 = jnp.float32
BF16 = jnp.bfloat16

epsilon = 1e-06
gate_power = 8.0
LANES = 128
COLS = 512
GROUP = 4
FAR = 20
FAR_EDGE = "far"
NEAR_EDGE = "near"


def one_minus_exp(y):
    series = F32(1.0 / 362880)
    for k in (40320, 5040, 720, 120, 24, 6, 2, 1):
        series = series * y + F32(1.0 / k)
    return jnp.where(y > -0.5, -y * series, 1.0 - jnp.exp(y))


def softplus(x):
    u = jnp.exp(-jnp.abs(x))
    series = F32(1.0 / 11)
    for k in range(10, 0, -1):
        series = F32(1.0 / k) - series * u
    return jnp.maximum(x, 0.0) + jnp.where(u < 0.125, u * series, jnp.log(1.0 + u))


def gelu(x):
    inner = F32(math.sqrt(2.0 / math.pi)) * (x + F32(0.044715) * (x * x * x))
    return x * (0.5 * (1.0 + jnp.tanh(inner)))


def to_column(row, size):
    lanes = row.shape[1]
    here = lax.broadcasted_iota(jnp.int32, (size, lanes), 0)
    there = lax.broadcasted_iota(jnp.int32, (size, lanes), 1)
    return jnp.sum(jnp.where(here == there, row, 0.0), axis=1, keepdims=True)


def kernel(
    cfg,
    resid_hbm,
    branch_hbm,
    gate_hbm,
    taps_hbm,
    rate_w_hbm,
    input_w_hbm,
    base_hbm,
    extra_hbm,
    outw_hbm,
    gmix_hbm,
    gpre_hbm,
    gpost_hbm,
    ids_hbm,
    rw_hbm,
    gp_hbm,
    up_hbm,
    dp_hbm,
    out_ref,
    resid_ref,
    keep_ref,
    state_ref,
    last_keep,
    last_state,
    act_ref,
    halo_ref,
    sum_ref,
    sums_ref,
    bo_ref,
    tok_ref,
    w_ref,
    e_ref,
    after_ref,
    ffn_ref,
    pick_ref,
    o_ref,
    x_ref,
    on_ref,
    ob_ref,
    xb_ref,
    m_ref,
    xf_ref,
    hid_ref,
    y_ref,
    r_ref,
    moe_ref,
    branch_ref,
    gate_ref,
    taps_ref,
    rate_w_ref,
    input_w_ref,
    base_ref,
    extra_ref,
    gmix_ref,
    gpre_ref,
    gpost_ref,
    ids_ref,
    rw_ref,
    loc_sem,
    send_sem,
    recv_sem,
):
    nsp, nx, ny = cfg
    ntp = nx * ny
    sp = lax.axis_index("sp")
    tp = lax.axis_index("tp")
    my_x, my_y = lax.rem(tp, nx), lax.div(tp, nx)
    core = lax.rem(sp, 2)
    chan, positions = branch_hbm.shape
    blocks = positions // LANES
    toks, width = resid_hbm.shape
    cap = o_ref.shape[1]
    slots = nsp * cap
    col_steps = width // COLS

    def remote(src, dst, k, to_sp, to_tp):
        return pltpu.make_async_remote_copy(
            src_ref=src, dst_ref=dst, send_sem=send_sem.at[k], recv_sem=recv_sem.at[k],
            device_id=(to_sp, to_tp), device_id_type=MESH,
        )

    def got(ref, k):
        pltpu.make_async_copy(ref, ref, recv_sem.at[k]).wait()

    def sent(ref, k):
        pltpu.make_async_copy(ref, ref, send_sem.at[k]).wait()

    own = [
        pltpu.make_async_copy(outw_hbm, w_ref.at[my_y, my_x], loc_sem.at[0]),
        pltpu.make_async_copy(gp_hbm, e_ref.at[0, my_y, my_x], loc_sem.at[1]),
        pltpu.make_async_copy(up_hbm, e_ref.at[1, my_y, my_x], loc_sem.at[2]),
        pltpu.make_async_copy(dp_hbm, e_ref.at[2, my_y, my_x], loc_sem.at[3]),
        pltpu.make_async_copy(resid_hbm, resid_ref, loc_sem.at[4]),
    ]
    small = [
        pltpu.make_async_copy(source, target, loc_sem.at[5 + k])
        for k, (source, target) in enumerate((
            (branch_hbm, branch_ref), (taps_hbm, taps_ref), (rate_w_hbm, rate_w_ref),
            (input_w_hbm, input_w_ref), (base_hbm, base_ref), (extra_hbm, extra_ref),
            (gate_hbm, gate_ref), (ids_hbm, ids_ref), (rw_hbm, rw_ref),
            (gmix_hbm, gmix_ref), (gpre_hbm, gpre_ref), (gpost_hbm, gpost_ref),
        ))
    ]
    for copy in small + own:
        copy.start()

    barrier = pltpu.get_barrier_semaphore()

    def greet_sp(k, carry):
        pl.semaphore_signal(
            barrier, inc=1, device_id=(lax.rem(sp + k, nsp), tp), device_id_type=MESH
        )
        return carry

    def greet_tp(k, carry):
        pl.semaphore_signal(
            barrier, inc=1, device_id=(sp, lax.rem(tp + k, ntp)), device_id_type=MESH
        )
        return carry

    lax.fori_loop(1, nsp, greet_sp, 0)
    lax.fori_loop(1, ntp, greet_tp, 0)

    for copy in small[:6]:
        copy.wait()

    taps = taps_ref[...].astype(F32)
    tap_cols = [to_column(taps[j : j + 1, :], chan) for j in range(4)]
    decay_rate = -gate_power * softplus(-to_column(base_ref[...], chan))
    lane = lax.broadcasted_iota(jnp.int32, (chan, LANES), 1)

    def lanes_of(index):
        return pl.ds(pl.multiple_of(index * LANES, LANES), LANES)

    def block_group(first, count, before):
        convs = []
        for g in range(count):
            cur = branch_ref[:, lanes_of(first + g)].astype(F32)
            total = tap_cols[3] * cur
            for back in (1, 2, 3):
                moved = jnp.where(
                    lane < back, pltpu.roll(before, back, 1), pltpu.roll(cur, back, 1)
                )
                total = total + tap_cols[3 - back] * moved
            convs.append(total)
            before = cur
        conv = jnp.concatenate(convs, axis=1)
        high = conv.astype(BF16)
        rest = conv - high.astype(F32)
        mid = rest.astype(BF16)
        low = (rest - mid.astype(F32)).astype(BF16)

        def gate_of(weight_ref):
            w = weight_ref[...]
            total = None
            for piece in (low, mid, high):
                part = lax.dot_general(
                    w, piece, (((0,), (0,)), ((), ())), preferred_element_type=F32
                )
                total = part if total is None else total + part
            return jax.nn.sigmoid(total)

        rate_gate = gate_of(rate_w_ref)
        input_gate = gate_of(input_w_ref)
        for g in range(count):
            at = slice(g * LANES, (g + 1) * LANES)
            extra = extra_ref[pl.ds(first + g, 1), :]
            log_keep = decay_rate * rate_gate[:, at] + extra
            keep = jnp.exp(log_keep)
            state = jnp.sqrt(one_minus_exp(2.0 * log_keep)) * input_gate[:, at] * convs[g]
            step = 1
            while step < LANES:
                inside = lane >= step
                keep_back = jnp.where(inside, pltpu.roll(keep, step, 1), 1.0)
                state_back = jnp.where(inside, pltpu.roll(state, step, 1), 0.0)
                state = keep * state_back + state
                keep = keep * keep_back
                step *= 2
            keep_ref[first + g] = keep
            state_ref[first + g] = state
            last_keep[first + g] = jnp.broadcast_to(keep[:, LANES - 1 :], (chan, LANES))
            last_state[first + g] = jnp.broadcast_to(state[:, LANES - 1 :], (chan, LANES))

    group = min(GROUP, blocks)

    def later_group(index, carry):
        first = index * group
        block_group(first, group, branch_ref[:, lanes_of(first - 1)].astype(F32))
        return carry

    lax.fori_loop(1, blocks // group, later_group, 0)
    block_group(1, group - 1, branch_ref[:, lanes_of(0)].astype(F32))

    for copy in small[6:]:
        copy.wait()

    def activate(index, carry):
        act_ref[index] = gelu(gate_ref[:, lanes_of(index)].astype(F32))
        return carry

    lax.fori_loop(0, blocks, activate, 0)

    ids = ids_ref[...]
    expert = lax.broadcasted_iota(jnp.int32, (nsp, toks), 0)
    named = [expert == ids[k : k + 1, :] for k in range(2)]
    counts = (named[0] | named[1]).astype(F32)
    token_a = lax.broadcasted_iota(jnp.int32, (toks, toks), 0)
    token_b = lax.broadcasted_iota(jnp.int32, (toks, toks), 1)
    earlier = jnp.dot(
        counts.astype(BF16), (token_a < token_b).astype(F32).astype(BF16),
        preferred_element_type=F32,
    )
    slot_at = [
        jnp.sum(
            jnp.where(named[k], earlier + (expert * cap).astype(F32), 0.0), axis=0, keepdims=True
        ).astype(jnp.int32)
        for k in range(2)
    ]
    slot = lax.broadcasted_iota(jnp.int32, (slots, toks), 0)
    chosen = [slot == slot_at[k] for k in range(2)]
    pick_ref[0] = (chosen[0] | chosen[1]).astype(F32).astype(BF16)
    weight = jnp.where(chosen[0], rw_ref[0:1, :], 0.0) + jnp.where(chosen[1], rw_ref[1:2, :], 0.0)
    weight_high = weight.astype(BF16)
    pick_ref[1] = weight_high
    pick_ref[2] = (weight - weight_high.astype(F32)).astype(BF16)

    own[4].wait()

    def cols_of(index):
        return pl.ds(pl.multiple_of(index * COLS, COLS), COLS)

    def spread(rows_ref, slots_ref):
        def some(index, carry):
            cols = cols_of(index)
            slots_ref[:, :, cols] = (
                jnp.dot(pick_ref[0], rows_ref[:, cols], preferred_element_type=F32)
                .astype(BF16)
                .reshape(nsp, cap, COLS)
            )
            return carry

        lax.fori_loop(0, col_steps, some, 0)

    spread(resid_ref, o_ref)

    far = nsp * FAR // 32

    def peer(k):
        away = lax.div(k + 1, 2)
        return lax.rem(lax.rem(k, 2) * away + (1 - lax.rem(k, 2)) * (nsp - away) + sp, nsp)

    if (far // 2) % 4 == 2:
        reach = nsp - far // 2 + lax.rem(lax.div(sp, 2), 2) * far
        ahead, behind = lax.rem(sp + nsp - reach + nsp, nsp), lax.rem(sp + reach, nsp)
        from_far, from_near = ahead, behind
    else:
        ahead, behind = peer(far - 1), peer(far)
        from_far, from_near = behind, ahead

    def send_block(source, target, sem, k, place):
        to = ahead if k is FAR_EDGE else behind if k is NEAR_EDGE else peer(k)
        remote(source.at[to], target.at[place], sem, to, tp).start()

    def send_blocks(source, target, sem, begin, end, offset=0):
        def step(k, carry):
            send_block(source, target, sem, k, k + 2 * lax.rem(k, 2) - 1 - offset)
            return carry

        lax.fori_loop(begin, end, step, 0)

    first_batch = min(far + 2, nsp - 1)

    pl.semaphore_wait(barrier, nsp - 1 + ntp - 1)
    remote(
        branch_ref.at[:, pl.ds(positions - LANES, LANES)], halo_ref, 0, lax.rem(sp + 1, nsp), tp
    ).start()

    send_block(o_ref, x_ref, 14, FAR_EDGE, far)
    send_blocks(o_ref, x_ref, 14, far + 1, first_batch)

    own[0].wait()
    half_a, half_b = 2 * core, 2 * core + 1

    def tp_at(y, x):
        return lax.rem(y, ny) * nx + lax.rem(x, nx)

    for k in range(1, nx):
        ref = w_ref.at[my_y, my_x, half_a]
        remote(ref, ref, 1, sp, tp_at(my_y, my_x + k)).start()
    for k in range(1, ny):
        ref = w_ref.at[my_y, my_x, half_b]
        remote(ref, ref, 2, sp, tp_at(my_y + k, my_x)).start()

    for copy in own[1:4]:
        copy.wait()
    for k in range(1, nx):
        ref = e_ref.at[:, my_y, my_x, 0]
        remote(ref, ref, 8, sp, tp_at(my_y, my_x + k)).start()
    for k in range(1, ny):
        ref = e_ref.at[:, my_y, my_x, 1]
        remote(ref, ref, 9, sp, tp_at(my_y + k, my_x)).start()

    got(halo_ref, 0)
    block_group(0, 1, jnp.where(sp == 0, 0.0, halo_ref[...].astype(F32)))

    def chain(index, carry):
        keep, state = carry
        block_keep, block_state = last_keep[index], last_state[index]
        last_keep[index] = keep
        last_state[index] = state
        return (block_keep * keep, block_keep * state + block_state)

    all_keep, all_state = lax.fori_loop(
        0, blocks, chain, (jnp.ones((chan, LANES), F32), jnp.zeros((chan, LANES), F32))
    )
    row = lax.broadcasted_iota(jnp.int32, (chan, LANES), 0)
    summary = jnp.where(lane == row, all_keep, 0.0) + jnp.where(
        lane == row + chan, all_state, 0.0
    )
    sum_ref[...] = jnp.sum(summary, axis=0, keepdims=True)
    sums_ref[sp] = sum_ref[...]

    def send_summary(k, carry):
        remote(sum_ref, sums_ref.at[sp], 5, lax.rem(sp + k, nsp), tp).start()
        return carry

    lax.fori_loop(1, nsp, send_summary, 0)
    send_blocks(o_ref, x_ref, 14, first_batch, nsp - 1)
    send_block(o_ref, x_ref, 14, nsp - 1, nsp - 1)

    got(w_ref.at[0, pl.ds(0, nx - 1), 0], 1)
    for k in range(1, ny):
        ref = w_ref.at[my_y, :, half_a]
        remote(ref, ref, 3, sp, tp_at(my_y + k, my_x)).start()
    got(w_ref.at[pl.ds(0, ny - 1), 0, 0], 2)
    for k in range(1, nx):
        ref = w_ref.at[:, my_x, half_b]
        remote(ref, ref, 4, sp, tp_at(my_y, my_x + k)).start()

    got(sums_ref.at[pl.ds(0, nsp - 1)], 5)

    def fold(index, carry):
        line = sums_ref[index]
        keep = jnp.where(index < sp, to_column(line, chan), 1.0)
        moved = jnp.where(
            index < sp,
            jnp.sum(jnp.where(lane == row + chan, line, 0.0), axis=1, keepdims=True),
            0.0,
        )
        return keep * carry + moved

    entering = lax.fori_loop(0, nsp, fold, jnp.zeros((chan, 1), F32), unroll=True)

    def finish(index, carry):
        begin = last_state[index] + last_keep[index] * entering
        hidden = state_ref[index] + keep_ref[index] * begin
        bo_ref[index] = (hidden * act_ref[index]).astype(BF16)
        return carry

    lax.fori_loop(0, blocks, finish, 0)

    def send_tokens(k, carry):
        to = lax.rem(tp + k, ntp)
        remote(bo_ref.at[to], tok_ref.at[tp], 6, sp, to).start()
        return carry

    lax.fori_loop(1, ntp, send_tokens, 0)
    tok_ref[tp] = bo_ref[tp]

    got(e_ref.at[:, 0, pl.ds(0, nx - 1), 0], 8)
    got(e_ref.at[:, pl.ds(0, ny - 1), 0, 1], 9)
    for a in range(3):
        for k in sorted({1, ny - 1}):
            ref = e_ref.at[a, my_y, :, 0]
            remote(ref, ref, 18 + a, sp, tp_at(my_y + k, my_x)).start()
        for k in sorted({1, nx - 1}):
            ref = e_ref.at[a, :, my_x, 1]
            remote(ref, ref, 21 + a, sp, tp_at(my_y, my_x + k)).start()

    got(w_ref.at[pl.ds(0, ny - 1), :, 0], 3)
    got(w_ref.at[:, pl.ds(0, nx - 1), 0], 4)
    ref = w_ref.at[:, :, pl.ds(2 * core, 2)]
    remote(ref, ref, 7, sp + 1 - 2 * core, tp).start()

    got(tok_ref.at[pl.ds(0, ntp - 1)], 6)
    ob_ref[...] = (
        lax.dot_general(
            pick_ref[0], tok_ref[...].reshape(ntp * chan, toks), (((1,), (1,)), ((), ())),
            preferred_element_type=F32,
        )
        .astype(BF16)
        .reshape(nsp, cap, ntp * chan)
    )
    send_block(ob_ref, xb_ref, 15, FAR_EDGE, 0)
    send_blocks(ob_ref, xb_ref, 15, far + 1, nsp - 1, far)
    send_block(ob_ref, xb_ref, 15, nsp - 1, nsp - 1 - far)

    got(w_ref.at[:, :, pl.ds(0, 2)], 7)

    def scale(values):
        return lax.rsqrt(jnp.mean(values * values, axis=-1, keepdims=True) + epsilon)

    def rows_of(index):
        return pl.ds(pl.multiple_of(index * 16, 16), 16)

    def projection(cols):
        return w_ref[:, :, :, :, cols].reshape(ntp * chan, COLS)

    def mix(index, carry):
        cols = cols_of(index)
        rows = tok_ref[...].reshape(ntp * chan, toks)
        moe_ref[:, cols] = lax.dot_general(
            rows, projection(cols), (((0,), (0,)), ((), ())), preferred_element_type=F32
        )
        return carry

    lax.fori_loop(0, col_steps, mix, 0)

    def norms(index, carry):
        rows = rows_of(index)
        mixed = moe_ref[rows, :]
        after = resid_ref[rows, :].astype(F32) + mixed * scale(mixed) * gmix_ref[...]
        after_ref[rows, :] = after
        ffn_ref[rows, :] = (after * scale(after) * gpre_ref[...]).astype(BF16)
        return carry

    lax.fori_loop(0, toks // 16, norms, 0, unroll=2)

    spread(ffn_ref, on_ref)
    send_blocks(on_ref, x_ref, 10, 1, far - 1)
    send_block(on_ref, x_ref, 10, NEAR_EDGE, far - 1)
    x_ref[0] = on_ref[sp]

    near_y, near_x = min(2, ny - 1), min(2, nx - 1)
    low, high = pl.ds(0, width // 2), pl.ds(width // 2, width // 2)
    for a in range(3):
        got(e_ref.at[a, pl.ds(0, near_y), :, 0], 18 + a)
        if ny > 2:
            before, after = lax.rem(my_y + ny - 1, ny), lax.rem(my_y + 1, ny)
            ref = e_ref.at[a, before, :, 0, :, low]
            remote(ref, ref, 24 + a, sp, tp_at(after, my_x)).start()
            ref = e_ref.at[a, after, :, 0, :, high]
            remote(ref, ref, 24 + a, sp, tp_at(before, my_x)).start()
        got(e_ref.at[a, :, pl.ds(0, near_x), 1], 21 + a)
        if nx > 2:
            before, after = lax.rem(my_x + nx - 1, nx), lax.rem(my_x + 1, nx)
            ref = e_ref.at[a, :, before, 1, :, low]
            remote(ref, ref, 27 + a, sp, tp_at(my_y, after)).start()
            ref = e_ref.at[a, :, after, 1, :, high]
            remote(ref, ref, 27 + a, sp, tp_at(my_y, before)).start()

    def whole_weights(a):
        if ny > 2:
            got(e_ref.at[a, 0, :, 0], 24 + a)
        if nx > 2:
            got(e_ref.at[a, :, 0, 1], 27 + a)

    per_y = nx * 32
    nt = (((1,), (1,)), ((), ()))
    sources = max(16 // cap, 1)

    def rows_at(index):
        count = sources * cap
        return pl.ds(pl.multiple_of(index * count, count), count)

    def blocks_at(base, index):
        return x_ref[pl.ds(base + index * sources, sources)].reshape(sources * cap, width)

    def serve(base, end, first):
        rows = (end - base) * cap
        if first:
            whole_weights(0)
            whole_weights(1)

        def expert_in(index, carry):
            ys = pl.ds(index * 2, 2)
            gate_rows = e_ref[0, ys].reshape(2 * per_y, width)
            up_rows = e_ref[1, ys].reshape(2 * per_y, width)
            inputs = xf_ref[0:rows, :]
            gate_vals = lax.dot_general(inputs, gate_rows, nt, preferred_element_type=F32)
            up_vals = lax.dot_general(inputs, up_rows, nt, preferred_element_type=F32)
            hid_ref[index, 0:rows, :] = (
                gate_vals * jax.nn.sigmoid(gate_vals) * up_vals
            ).astype(BF16)
            return carry

        lax.fori_loop(0, ny // 2, expert_in, 0)

        if first:
            whole_weights(2)

        def expert_out(index, carry):
            cols = cols_of(index)
            total = None
            for pair in range(ny // 2):
                down = e_ref[2, 2 * pair : 2 * pair + 2, :, :, :, cols].reshape(2 * per_y, COLS)
                product = jnp.dot(hid_ref[pair, 0:rows, :], down, preferred_element_type=F32)
                total = product if total is None else total + product
            y_ref[base:end, :, cols] = total.astype(BF16).reshape(end - base, cap, COLS)
            return carry

        lax.fori_loop(0, col_steps, expert_out, 0)

        def give_back(k, carry):
            remote(y_ref.at[k], r_ref.at[sp], 13, peer(k), tp).start()
            return carry

        if first:
            lax.fori_loop(far + 1, nsp, give_back, 0)
            remote(y_ref.at[far], r_ref.at[sp], 13, from_far, tp).start()
        else:
            lax.fori_loop(1, far - 1, give_back, 0)
            remote(y_ref.at[far - 1], r_ref.at[sp], 13, from_near, tp).start()

    got(x_ref.at[pl.ds(0, nsp - far)], 14)
    got(xb_ref, 15)

    def mix_arrived(index, carry):
        cols = cols_of(index)
        m_ref[:, cols] = jnp.dot(
            xb_ref[...].reshape((nsp - far) * cap, ntp * chan), projection(cols),
            preferred_element_type=F32,
        )
        return carry

    lax.fori_loop(0, col_steps, mix_arrived, 0)

    def norm_arrived(index, carry):
        rows = rows_at(index)
        mixed = m_ref[rows, :]
        after = (
            blocks_at(far, index).astype(F32) + mixed * scale(mixed) * gmix_ref[...]
        )
        xf_ref[rows, :] = (after * scale(after) * gpre_ref[...]).astype(BF16)
        return carry

    lax.fori_loop(0, (nsp - far) // sources, norm_arrived, 0, unroll=2)
    serve(far, nsp, True)

    got(x_ref.at[pl.ds(0, far - 1)], 10)

    def take_arrived(index, carry):
        xf_ref[rows_at(index), :] = blocks_at(0, index)
        return carry

    lax.fori_loop(0, far // sources, take_arrived, 0)
    serve(0, far, False)
    r_ref[sp] = y_ref[0]
    got(r_ref.at[pl.ds(0, nsp - 1)], 13)

    def combine(index, carry):
        cols = cols_of(index)
        rows = r_ref[:, :, cols].reshape(slots, COLS)
        tn = (((0,), (0,)), ((), ()))
        moe_ref[:, cols] = lax.dot_general(
            pick_ref[2], rows, tn, preferred_element_type=F32
        ) + lax.dot_general(pick_ref[1], rows, tn, preferred_element_type=F32)
        return carry

    lax.fori_loop(0, col_steps, combine, 0)

    def finalize(index, carry):
        rows = rows_of(index)
        moe = moe_ref[rows, :]
        out_ref[rows, :] = (after_ref[rows, :] + moe * scale(moe) * gpost_ref[...]).astype(BF16)
        return carry

    lax.fori_loop(0, toks // 16, finalize, 0, unroll=2)

    sent(halo_ref, 0)
    sent(w_ref.at[0, pl.ds(0, nx - 1), 0], 1)
    sent(w_ref.at[pl.ds(0, ny - 1), 0, 0], 2)
    sent(w_ref.at[pl.ds(0, ny - 1), :, 0], 3)
    sent(w_ref.at[:, pl.ds(0, nx - 1), 0], 4)
    sent(sums_ref.at[pl.ds(0, nsp - 1)], 5)
    sent(tok_ref.at[pl.ds(0, ntp - 1)], 6)
    sent(w_ref.at[:, :, pl.ds(0, 2)], 7)
    sent(e_ref.at[:, 0, pl.ds(0, nx - 1), 0], 8)
    sent(e_ref.at[:, pl.ds(0, ny - 1), 0, 1], 9)
    sent(x_ref.at[pl.ds(0, far - 1)], 10)
    sent(x_ref.at[pl.ds(0, nsp - far)], 14)
    sent(xb_ref, 15)
    for a in range(3):
        sent(e_ref.at[a, pl.ds(0, near_y), :, 0], 18 + a)
        sent(e_ref.at[a, :, pl.ds(0, near_x), 1], 21 + a)
        if ny > 2:
            sent(e_ref.at[a, 0, :, 0], 24 + a)
        if nx > 2:
            sent(e_ref.at[a, :, 0, 1], 27 + a)
    sent(r_ref.at[pl.ds(0, nsp - 1)], 13)


def solution(mesh):
    nsp, ntp = mesh.shape["sp"], mesh.shape["tp"]
    nx = math.isqrt(ntp)
    ny = ntp // nx

    def per_device(
        resid, branch_input, gate_in, conv_taps, rate_weight, input_weight, decay_base,
        decay_extra, out_weight, gain_mix, gain_pre, gain_post, expert_ids, route_weight,
        gate_proj, up_proj, down_proj,
    ):
        chan, positions = branch_input.shape
        toks, width = resid.shape
        blocks = positions // LANES
        cap = 2 * toks // nsp
        vmem = pl.BlockSpec(memory_space=pltpu.VMEM)
        hbm = pl.BlockSpec(memory_space=pltpu.HBM)
        block = (blocks, chan, LANES)
        far = nsp * FAR // 32
        return pl.pallas_call(
            functools.partial(kernel, (nsp, nx, ny)),
            out_shape=jax.ShapeDtypeStruct((toks, width), BF16),
            in_specs=[hbm] * 17,
            out_specs=vmem,
            scratch_shapes=[
                pltpu.VMEM((toks, width), BF16),
                pltpu.VMEM(block, F32),
                pltpu.VMEM(block, F32),
                pltpu.VMEM(block, F32),
                pltpu.VMEM(block, F32),
                pltpu.VMEM(block, F32),
                pltpu.VMEM((chan, LANES), BF16),
                pltpu.VMEM((1, LANES), F32),
                pltpu.VMEM((nsp, 1, LANES), F32),
                pltpu.VMEM(block, BF16),
                pltpu.VMEM((ntp, chan, toks), BF16),
                pltpu.VMEM((ny, nx, 4, chan // 4, width), BF16),
                pltpu.VMEM((3, ny, nx, 2, 16, width), BF16),
                pltpu.VMEM((toks, width), F32),
                pltpu.VMEM((toks, width), BF16),
                pltpu.VMEM((3, nsp * cap, toks), BF16),
                pltpu.VMEM((nsp, cap, width), BF16),
                pltpu.VMEM((nsp, cap, width), BF16),
                pltpu.VMEM((nsp, cap, width), BF16),
                pltpu.VMEM((nsp, cap, ntp * chan), BF16),
                pltpu.VMEM((nsp - far, cap, ntp * chan), BF16),
                pltpu.VMEM(((nsp - far) * cap, width), F32),
                pltpu.VMEM((max(far, nsp - far) * cap, width), BF16),
                pltpu.VMEM((ny // 2, max(far, nsp - far) * cap, nx * 64), BF16),
                pltpu.VMEM((nsp, cap, width), BF16),
                pltpu.VMEM((nsp, cap, width), BF16),
                pltpu.VMEM((toks, width), F32),
                pltpu.VMEM((chan, positions), BF16),
                pltpu.VMEM((chan, positions), BF16),
                pltpu.VMEM(conv_taps.shape, BF16),
                pltpu.VMEM((chan, chan), BF16),
                pltpu.VMEM((chan, chan), BF16),
                pltpu.VMEM((1, chan), F32),
                pltpu.VMEM((blocks, LANES), F32),
                pltpu.VMEM((1, width), F32),
                pltpu.VMEM((1, width), F32),
                pltpu.VMEM((1, width), F32),
                pltpu.VMEM((2, toks), jnp.int32),
                pltpu.VMEM((2, toks), F32),
                pltpu.SemaphoreType.DMA((17,)),
                pltpu.SemaphoreType.DMA((30,)),
                pltpu.SemaphoreType.DMA((30,)),
            ],
            compiler_params=pltpu.CompilerParams(
                collective_id=0, has_side_effects=True, vmem_limit_bytes=67043328
            ),
        )(
            resid, branch_input, gate_in, conv_taps,
            rate_weight.reshape(chan, chan), input_weight.reshape(chan, chan),
            decay_base.reshape(1, chan), decay_extra.reshape(blocks, LANES),
            out_weight.reshape(4, chan // 4, width),
            gain_mix.reshape(1, width), gain_pre.reshape(1, width), gain_post.reshape(1, width),
            expert_ids.T, route_weight.T,
            gate_proj.reshape(2, 16, width), up_proj.reshape(2, 16, width),
            down_proj.reshape(2, 16, width),
        )

    sp_tp = P(("sp", "tp"), None)
    experts = P("sp", "tp", None)
    return jax.shard_map(
        per_device,
        mesh=mesh,
        in_specs=(
            sp_tp, P("tp", "sp"), P("tp", "sp"), P(None, "tp"),
            P("tp", None, None), P("tp", None, None), P("tp"), P("sp"), P("tp", None),
            P(), P(), P(), sp_tp, sp_tp, experts, experts, experts,
        ),
        out_specs=sp_tp,
        check_vma=False,
    )
```

```python
import functools
import math

import jax
import jax.numpy as jnp
from jax import lax
from jax.experimental import pallas as pl
from jax.experimental.pallas import tpu as pltpu
from jax.sharding import PartitionSpec as P

MESH = pl.DeviceIdType.MESH
F32 = jnp.float32
BF16 = jnp.bfloat16

epsilon = 1e-06
gate_power = 8.0
LANES = 128
COLS = 512
GROUP = 4
FAR = 22
FAR_EDGE = "far"
NEAR_EDGE = "near"


def one_minus_exp(y):
    series = F32(1.0 / 362880)
    for k in (40320, 5040, 720, 120, 24, 6, 2, 1):
        series = series * y + F32(1.0 / k)
    return jnp.where(y > -0.5, -y * series, 1.0 - jnp.exp(y))


def softplus(x):
    u = jnp.exp(-jnp.abs(x))
    series = F32(1.0 / 11)
    for k in range(10, 0, -1):
        series = F32(1.0 / k) - series * u
    return jnp.maximum(x, 0.0) + jnp.where(u < 0.125, u * series, jnp.log(1.0 + u))


def gelu(x):
    inner = F32(math.sqrt(2.0 / math.pi)) * (x + F32(0.044715) * (x * x * x))
    return x * (0.5 * (1.0 + jnp.tanh(inner)))


def to_column(row, size):
    lanes = row.shape[1]
    here = lax.broadcasted_iota(jnp.int32, (size, lanes), 0)
    there = lax.broadcasted_iota(jnp.int32, (size, lanes), 1)
    return jnp.sum(jnp.where(here == there, row, 0.0), axis=1, keepdims=True)


def kernel(
    cfg,
    resid_hbm,
    branch_hbm,
    gate_hbm,
    taps_hbm,
    rate_w_hbm,
    input_w_hbm,
    base_hbm,
    extra_hbm,
    outw_hbm,
    gmix_hbm,
    gpre_hbm,
    gpost_hbm,
    ids_hbm,
    rw_hbm,
    gp_hbm,
    up_hbm,
    dp_hbm,
    out_ref,
    resid_ref,
    keep_ref,
    state_ref,
    last_keep,
    last_state,
    act_ref,
    halo_ref,
    sum_ref,
    sums_ref,
    bo_ref,
    tok_ref,
    w_ref,
    e_ref,
    after_ref,
    ffn_ref,
    pick_ref,
    o_ref,
    x_ref,
    on_ref,
    ob_ref,
    xb_ref,
    m_ref,
    xf_ref,
    hid_ref,
    y_ref,
    r_ref,
    moe_ref,
    branch_ref,
    gate_ref,
    taps_ref,
    rate_w_ref,
    input_w_ref,
    base_ref,
    extra_ref,
    gmix_ref,
    gpre_ref,
    gpost_ref,
    ids_ref,
    rw_ref,
    loc_sem,
    send_sem,
    recv_sem,
):
    nsp, nx, ny = cfg
    ntp = nx * ny
    sp = lax.axis_index("sp")
    tp = lax.axis_index("tp")
    my_x, my_y = lax.rem(tp, nx), lax.div(tp, nx)
    core = lax.rem(sp, 2)
    chan, positions = branch_hbm.shape
    blocks = positions // LANES
    toks, width = resid_hbm.shape
    cap = o_ref.shape[1]
    slots = nsp * cap
    col_steps = width // COLS

    def remote(src, dst, k, to_sp, to_tp):
        return pltpu.make_async_remote_copy(
            src_ref=src, dst_ref=dst, send_sem=send_sem.at[k], recv_sem=recv_sem.at[k],
            device_id=(to_sp, to_tp), device_id_type=MESH,
        )

    def got(ref, k):
        pltpu.make_async_copy(ref, ref, recv_sem.at[k]).wait()

    def sent(ref, k):
        pltpu.make_async_copy(ref, ref, send_sem.at[k]).wait()

    barrier = pltpu.get_barrier_semaphore()

    def greet_sp(k, carry):
        pl.semaphore_signal(
            barrier, inc=1, device_id=(lax.rem(sp + k, nsp), tp), device_id_type=MESH
        )
        return carry

    def greet_tp(k, carry):
        pl.semaphore_signal(
            barrier, inc=1, device_id=(sp, lax.rem(tp + k, ntp)), device_id_type=MESH
        )
        return carry

    lax.fori_loop(1, nsp, greet_sp, 0)
    lax.fori_loop(1, ntp, greet_tp, 0)

    own = [
        pltpu.make_async_copy(outw_hbm, w_ref.at[my_y, my_x], loc_sem.at[0]),
        pltpu.make_async_copy(gp_hbm, e_ref.at[0, my_y, my_x], loc_sem.at[1]),
        pltpu.make_async_copy(up_hbm, e_ref.at[1, my_y, my_x], loc_sem.at[2]),
        pltpu.make_async_copy(dp_hbm, e_ref.at[2, my_y, my_x], loc_sem.at[3]),
        pltpu.make_async_copy(resid_hbm, resid_ref, loc_sem.at[4]),
    ]
    small = [
        pltpu.make_async_copy(source, target, loc_sem.at[5 + k])
        for k, (source, target) in enumerate((
            (branch_hbm, branch_ref), (taps_hbm, taps_ref), (rate_w_hbm, rate_w_ref),
            (input_w_hbm, input_w_ref), (base_hbm, base_ref), (extra_hbm, extra_ref),
            (gate_hbm, gate_ref), (ids_hbm, ids_ref), (rw_hbm, rw_ref),
            (gmix_hbm, gmix_ref), (gpre_hbm, gpre_ref), (gpost_hbm, gpost_ref),
        ))
    ]
    for copy in small + own:
        copy.start()

    for copy in small[:6]:
        copy.wait()

    taps = taps_ref[...].astype(F32)
    tap_cols = [to_column(taps[j : j + 1, :], chan) for j in range(4)]
    decay_rate = -gate_power * softplus(-to_column(base_ref[...], chan))
    lane = lax.broadcasted_iota(jnp.int32, (chan, LANES), 1)

    def lanes_of(index):
        return pl.ds(pl.multiple_of(index * LANES, LANES), LANES)

    def block_group(first, count, before):
        convs = []
        for g in range(count):
            cur = branch_ref[:, lanes_of(first + g)].astype(F32)
            total = tap_cols[3] * cur
            for back in (1, 2, 3):
                moved = jnp.where(
                    lane < back, pltpu.roll(before, back, 1), pltpu.roll(cur, back, 1)
                )
                total = total + tap_cols[3 - back] * moved
            convs.append(total)
            before = cur
        conv = jnp.concatenate(convs, axis=1)
        high = conv.astype(BF16)
        rest = conv - high.astype(F32)
        mid = rest.astype(BF16)
        low = (rest - mid.astype(F32)).astype(BF16)

        def gate_of(weight_ref):
            w = weight_ref[...]
            total = None
            for piece in (low, mid, high):
                part = lax.dot_general(
                    w, piece, (((0,), (0,)), ((), ())), preferred_element_type=F32
                )
                total = part if total is None else total + part
            return jax.nn.sigmoid(total)

        rate_gate = gate_of(rate_w_ref)
        input_gate = gate_of(input_w_ref)
        for g in range(count):
            at = slice(g * LANES, (g + 1) * LANES)
            extra = extra_ref[pl.ds(first + g, 1), :]
            log_keep = decay_rate * rate_gate[:, at] + extra
            keep = jnp.exp(log_keep)
            state = jnp.sqrt(one_minus_exp(2.0 * log_keep)) * input_gate[:, at] * convs[g]
            step = 1
            while step < LANES:
                inside = lane >= step
                keep_back = jnp.where(inside, pltpu.roll(keep, step, 1), 1.0)
                state_back = jnp.where(inside, pltpu.roll(state, step, 1), 0.0)
                state = keep * state_back + state
                keep = keep * keep_back
                step *= 2
            keep_ref[first + g] = keep
            state_ref[first + g] = state
            last_keep[first + g] = jnp.broadcast_to(keep[:, LANES - 1 :], (chan, LANES))
            last_state[first + g] = jnp.broadcast_to(state[:, LANES - 1 :], (chan, LANES))

    group = min(GROUP, blocks)

    def later_group(index, carry):
        first = index * group
        block_group(first, group, branch_ref[:, lanes_of(first - 1)].astype(F32))
        return carry


    for copy in small[6:]:
        copy.wait()

    ids = ids_ref[...]
    expert = lax.broadcasted_iota(jnp.int32, (nsp, toks), 0)
    named = [expert == ids[k : k + 1, :] for k in range(2)]
    counts = (named[0] | named[1]).astype(F32)
    token_a = lax.broadcasted_iota(jnp.int32, (toks, toks), 0)
    token_b = lax.broadcasted_iota(jnp.int32, (toks, toks), 1)
    earlier = jnp.dot(
        counts.astype(BF16), (token_a < token_b).astype(F32).astype(BF16),
        preferred_element_type=F32,
    )
    slot_at = [
        jnp.sum(
            jnp.where(named[k], earlier + (expert * cap).astype(F32), 0.0), axis=0, keepdims=True
        ).astype(jnp.int32)
        for k in range(2)
    ]
    slot = lax.broadcasted_iota(jnp.int32, (slots, toks), 0)
    chosen = [slot == slot_at[k] for k in range(2)]
    pick_ref[0] = (chosen[0] | chosen[1]).astype(F32).astype(BF16)
    weight = jnp.where(chosen[0], rw_ref[0:1, :], 0.0) + jnp.where(chosen[1], rw_ref[1:2, :], 0.0)
    weight_high = weight.astype(BF16)
    pick_ref[1] = weight_high
    pick_ref[2] = (weight - weight_high.astype(F32)).astype(BF16)

    own[4].wait()

    def cols_of(index):
        return pl.ds(pl.multiple_of(index * COLS, COLS), COLS)

    def spread(rows_ref, slots_ref):
        def some(index, carry):
            cols = cols_of(index)
            slots_ref[:, :, cols] = (
                jnp.dot(pick_ref[0], rows_ref[:, cols], preferred_element_type=F32)
                .astype(BF16)
                .reshape(nsp, cap, COLS)
            )
            return carry

        lax.fori_loop(0, col_steps, some, 0)

    spread(resid_ref, o_ref)

    far = nsp * FAR // 32

    def peer(k):
        away = lax.div(k + 1, 2)
        return lax.rem(lax.rem(k, 2) * away + (1 - lax.rem(k, 2)) * (nsp - away) + sp, nsp)

    if (far // 2) % 4 == 2:
        reach = nsp - far // 2 + lax.rem(lax.div(sp, 2), 2) * far
        ahead, behind = lax.rem(sp + nsp - reach + nsp, nsp), lax.rem(sp + reach, nsp)
        from_far, from_near = ahead, behind
    else:
        ahead, behind = peer(far - 1), peer(far)
        from_far, from_near = behind, ahead

    def send_block(source, target, sem, k, place):
        to = ahead if k is FAR_EDGE else behind if k is NEAR_EDGE else peer(k)
        remote(source.at[to], target.at[place], sem, to, tp).start()

    def send_blocks(source, target, sem, begin, end, offset=0):
        def step(k, carry):
            send_block(source, target, sem, k, k + 2 * lax.rem(k, 2) - 1 - offset)
            return carry

        lax.fori_loop(begin, end, step, 0)

    first_batch = min(far + 2, nsp - 1)

    early_groups = min(2, blocks // group)
    lax.fori_loop(early_groups + 1, blocks // group, later_group, 0)

    pl.semaphore_wait(barrier, nsp - 1 + ntp - 1)
    remote(
        branch_ref.at[:, pl.ds(positions - LANES, LANES)], halo_ref, 0, lax.rem(sp + 1, nsp), tp
    ).start()

    send_block(o_ref, x_ref, 14, FAR_EDGE, far)
    send_blocks(o_ref, x_ref, 14, far + 1, first_batch)

    own[0].wait()
    half_a, half_b = 2 * core, 2 * core + 1

    def tp_at(y, x):
        return lax.rem(y, ny) * nx + lax.rem(x, nx)

    for k in range(1, nx):
        ref = w_ref.at[my_y, my_x, half_a]
        remote(ref, ref, 1, sp, tp_at(my_y, my_x + k)).start()
    for k in range(1, ny):
        ref = w_ref.at[my_y, my_x, half_b]
        remote(ref, ref, 2, sp, tp_at(my_y + k, my_x)).start()

    for copy in own[1:4]:
        copy.wait()
    for k in range(1, nx):
        ref = e_ref.at[0, my_y, my_x, 0]
        remote(ref, ref, 8, sp, tp_at(my_y, my_x + k)).start()
    for k in range(1, ny):
        ref = e_ref.at[0, my_y, my_x, 1]
        remote(ref, ref, 9, sp, tp_at(my_y + k, my_x)).start()

    lax.fori_loop(1, min(early_groups + 1, blocks // group), later_group, 0)
    block_group(1, group - 1, branch_ref[:, lanes_of(0)].astype(F32))
    got(halo_ref, 0)
    block_group(0, 1, jnp.where(sp == 0, 0.0, halo_ref[...].astype(F32)))

    def chain(index, carry):
        keep, state = carry
        block_keep, block_state = last_keep[index], last_state[index]
        last_keep[index] = keep
        last_state[index] = state
        return (block_keep * keep, block_keep * state + block_state)

    all_keep, all_state = lax.fori_loop(
        0, blocks, chain, (jnp.ones((chan, LANES), F32), jnp.zeros((chan, LANES), F32))
    )
    row = lax.broadcasted_iota(jnp.int32, (chan, LANES), 0)
    summary = jnp.where(lane == row, all_keep, 0.0) + jnp.where(
        lane == row + chan, all_state, 0.0
    )
    sum_ref[...] = jnp.sum(summary, axis=0, keepdims=True)
    sums_ref[sp] = sum_ref[...]

    def send_summary(k, carry):
        remote(sum_ref, sums_ref.at[sp], 5, lax.rem(sp + k, nsp), tp).start()
        return carry

    lax.fori_loop(1, nsp, send_summary, 0)
    send_blocks(o_ref, x_ref, 14, first_batch, nsp - 1)
    send_block(o_ref, x_ref, 14, nsp - 1, nsp - 1)

    got(w_ref.at[0, pl.ds(0, nx - 1), 0], 1)
    for k in range(1, ny):
        ref = w_ref.at[my_y, :, half_a]
        remote(ref, ref, 3, sp, tp_at(my_y + k, my_x)).start()
    got(w_ref.at[pl.ds(0, ny - 1), 0, 0], 2)
    for k in range(1, nx):
        ref = w_ref.at[:, my_x, half_b]
        remote(ref, ref, 4, sp, tp_at(my_y, my_x + k)).start()

    def activate(index, carry):
        act_ref[index] = gelu(gate_ref[:, lanes_of(index)].astype(F32))
        return carry

    lax.fori_loop(0, blocks, activate, 0)

    got(sums_ref.at[pl.ds(0, nsp - 1)], 5)

    def fold(index, carry):
        line = sums_ref[index]
        keep = jnp.where(index < sp, to_column(line, chan), 1.0)
        moved = jnp.where(
            index < sp,
            jnp.sum(jnp.where(lane == row + chan, line, 0.0), axis=1, keepdims=True),
            0.0,
        )
        return keep * carry + moved

    entering = lax.fori_loop(0, nsp, fold, jnp.zeros((chan, 1), F32), unroll=True)

    def finish(index, carry):
        begin = last_state[index] + last_keep[index] * entering
        hidden = state_ref[index] + keep_ref[index] * begin
        bo_ref[index] = (hidden * act_ref[index]).astype(BF16)
        return carry

    lax.fori_loop(0, blocks, finish, 0)

    def send_tokens(k, carry):
        to = lax.rem(tp + k, ntp)
        remote(bo_ref.at[to], tok_ref.at[tp], 6, sp, to).start()
        return carry

    lax.fori_loop(1, ntp, send_tokens, 0)
    tok_ref[tp] = bo_ref[tp]

    for k in range(1, nx):
        ref = e_ref.at[pl.ds(1, 2), my_y, my_x, 0]
        remote(ref, ref, 11, sp, tp_at(my_y, my_x + k)).start()
    for k in range(1, ny):
        ref = e_ref.at[pl.ds(1, 2), my_y, my_x, 1]
        remote(ref, ref, 12, sp, tp_at(my_y + k, my_x)).start()

    def second_leg(a):
        for k in sorted({1, ny - 1}):
            ref = e_ref.at[a, my_y, :, 0]
            remote(ref, ref, 18 + a, sp, tp_at(my_y + k, my_x)).start()
        for k in sorted({1, nx - 1}):
            ref = e_ref.at[a, :, my_x, 1]
            remote(ref, ref, 21 + a, sp, tp_at(my_y, my_x + k)).start()

    got(e_ref.at[0, 0, pl.ds(0, nx - 1), 0], 8)
    got(e_ref.at[0, pl.ds(0, ny - 1), 0, 1], 9)
    second_leg(0)

    got(w_ref.at[pl.ds(0, ny - 1), :, 0], 3)
    got(w_ref.at[:, pl.ds(0, nx - 1), 0], 4)
    ref = w_ref.at[:, :, pl.ds(2 * core, 2)]
    remote(ref, ref, 7, sp + 1 - 2 * core, tp).start()

    got(tok_ref.at[pl.ds(0, ntp - 1)], 6)
    ob_ref[...] = (
        lax.dot_general(
            pick_ref[0], tok_ref[...].reshape(ntp * chan, toks), (((1,), (1,)), ((), ())),
            preferred_element_type=F32,
        )
        .astype(BF16)
        .reshape(nsp, cap, ntp * chan)
    )
    send_block(ob_ref, xb_ref, 15, FAR_EDGE, 0)
    send_blocks(ob_ref, xb_ref, 15, far + 1, nsp - 1, far)
    send_block(ob_ref, xb_ref, 15, nsp - 1, nsp - 1 - far)

    got(w_ref.at[:, :, pl.ds(0, 2)], 7)

    def scale(values):
        return lax.rsqrt(jnp.mean(values * values, axis=-1, keepdims=True) + epsilon)

    def rows_of(index):
        return pl.ds(pl.multiple_of(index * 16, 16), 16)

    def projection(cols):
        return w_ref[:, :, :, :, cols].reshape(ntp * chan, COLS)

    def mix(index, carry):
        cols = cols_of(index)
        rows = tok_ref[...].reshape(ntp * chan, toks)
        moe_ref[:, cols] = lax.dot_general(
            rows, projection(cols), (((0,), (0,)), ((), ())), preferred_element_type=F32
        )
        return carry

    lax.fori_loop(0, col_steps, mix, 0)

    def norms(index, carry):
        rows = rows_of(index)
        mixed = moe_ref[rows, :]
        after = resid_ref[rows, :].astype(F32) + mixed * scale(mixed) * gmix_ref[...]
        after_ref[rows, :] = after
        ffn_ref[rows, :] = (after * scale(after) * gpre_ref[...]).astype(BF16)
        return carry

    lax.fori_loop(0, toks // 16, norms, 0, unroll=2)

    spread(ffn_ref, on_ref)
    send_blocks(on_ref, x_ref, 10, 1, far - 1)
    send_block(on_ref, x_ref, 10, NEAR_EDGE, far - 1)
    x_ref[0] = on_ref[sp]

    got(e_ref.at[pl.ds(1, 2), 0, pl.ds(0, nx - 1), 0], 11)
    got(e_ref.at[pl.ds(1, 2), pl.ds(0, ny - 1), 0, 1], 12)
    second_leg(1)
    second_leg(2)
    near_y, near_x = min(2, ny - 1), min(2, nx - 1)
    low, high = pl.ds(0, width // 2), pl.ds(width // 2, width // 2)
    for a in range(3):
        got(e_ref.at[a, pl.ds(0, near_y), :, 0], 18 + a)
        if ny > 2:
            before, after = lax.rem(my_y + ny - 1, ny), lax.rem(my_y + 1, ny)
            ref = e_ref.at[a, before, :, 0, :, low]
            remote(ref, ref, 24 + a, sp, tp_at(after, my_x)).start()
            ref = e_ref.at[a, after, :, 0, :, high]
            remote(ref, ref, 24 + a, sp, tp_at(before, my_x)).start()
        got(e_ref.at[a, :, pl.ds(0, near_x), 1], 21 + a)
        if nx > 2:
            before, after = lax.rem(my_x + nx - 1, nx), lax.rem(my_x + 1, nx)
            ref = e_ref.at[a, :, before, 1, :, low]
            remote(ref, ref, 27 + a, sp, tp_at(my_y, after)).start()
            ref = e_ref.at[a, :, after, 1, :, high]
            remote(ref, ref, 27 + a, sp, tp_at(my_y, before)).start()

    def whole_weights(a):
        if ny > 2:
            got(e_ref.at[a, 0, :, 0], 24 + a)
        if nx > 2:
            got(e_ref.at[a, :, 0, 1], 27 + a)

    per_y = nx * 32
    nt = (((1,), (1,)), ((), ()))
    sources = max(16 // cap, 1)

    def rows_at(index):
        count = sources * cap
        return pl.ds(pl.multiple_of(index * count, count), count)

    def blocks_at(base, index):
        return x_ref[pl.ds(base + index * sources, sources)].reshape(sources * cap, width)

    def serve(base, end, first):
        rows = (end - base) * cap
        if first:
            whole_weights(0)
            whole_weights(1)

        def expert_in(index, carry):
            ys = pl.ds(index * 2, 2)
            gate_rows = e_ref[0, ys].reshape(2 * per_y, width)
            up_rows = e_ref[1, ys].reshape(2 * per_y, width)
            inputs = xf_ref[0:rows, :]
            gate_vals = lax.dot_general(inputs, gate_rows, nt, preferred_element_type=F32)
            up_vals = lax.dot_general(inputs, up_rows, nt, preferred_element_type=F32)
            hid_ref[index, 0:rows, :] = (
                gate_vals * jax.nn.sigmoid(gate_vals) * up_vals
            ).astype(BF16)
            return carry

        lax.fori_loop(0, ny // 2, expert_in, 0)

        if first:
            whole_weights(2)

        def expert_out(index, carry):
            cols = cols_of(index)
            total = None
            for pair in range(ny // 2):
                down = e_ref[2, 2 * pair : 2 * pair + 2, :, :, :, cols].reshape(2 * per_y, COLS)
                product = jnp.dot(hid_ref[pair, 0:rows, :], down, preferred_element_type=F32)
                total = product if total is None else total + product
            y_ref[base:end, :, cols] = total.astype(BF16).reshape(end - base, cap, COLS)
            return carry

        lax.fori_loop(0, col_steps, expert_out, 0)

        def give_back(k, carry):
            remote(y_ref.at[k], r_ref.at[sp], 13, peer(k), tp).start()
            return carry

        if first:
            lax.fori_loop(far + 1, nsp, give_back, 0)
            remote(y_ref.at[far], r_ref.at[sp], 13, from_far, tp).start()
        else:
            lax.fori_loop(1, far - 1, give_back, 0)
            remote(y_ref.at[far - 1], r_ref.at[sp], 13, from_near, tp).start()

    got(x_ref.at[pl.ds(0, nsp - far)], 14)
    got(xb_ref, 15)

    def mix_arrived(index, carry):
        cols = cols_of(index)
        m_ref[:, cols] = jnp.dot(
            xb_ref[...].reshape((nsp - far) * cap, ntp * chan), projection(cols),
            preferred_element_type=F32,
        )
        return carry

    lax.fori_loop(0, col_steps, mix_arrived, 0)

    def norm_arrived(index, carry):
        rows = rows_at(index)
        mixed = m_ref[rows, :]
        after = (
            blocks_at(far, index).astype(F32) + mixed * scale(mixed) * gmix_ref[...]
        )
        xf_ref[rows, :] = (after * scale(after) * gpre_ref[...]).astype(BF16)
        return carry

    lax.fori_loop(0, (nsp - far) // sources, norm_arrived, 0, unroll=2)
    serve(far, nsp, True)

    got(x_ref.at[pl.ds(0, far - 1)], 10)

    def take_arrived(index, carry):
        xf_ref[rows_at(index), :] = blocks_at(0, index)
        return carry

    lax.fori_loop(0, far // sources, take_arrived, 0)
    serve(0, far, False)
    r_ref[sp] = y_ref[0]
    got(r_ref.at[pl.ds(0, nsp - 1)], 13)

    def combine(index, carry):
        cols = cols_of(index)
        rows = r_ref[:, :, cols].reshape(slots, COLS)
        tn = (((0,), (0,)), ((), ()))
        moe_ref[:, cols] = lax.dot_general(
            pick_ref[2], rows, tn, preferred_element_type=F32
        ) + lax.dot_general(pick_ref[1], rows, tn, preferred_element_type=F32)
        return carry

    lax.fori_loop(0, col_steps, combine, 0)

    def finalize(index, carry):
        rows = rows_of(index)
        moe = moe_ref[rows, :]
        out_ref[rows, :] = (after_ref[rows, :] + moe * scale(moe) * gpost_ref[...]).astype(BF16)
        return carry

    lax.fori_loop(0, toks // 16, finalize, 0, unroll=2)

    sent(halo_ref, 0)
    sent(w_ref.at[0, pl.ds(0, nx - 1), 0], 1)
    sent(w_ref.at[pl.ds(0, ny - 1), 0, 0], 2)
    sent(w_ref.at[pl.ds(0, ny - 1), :, 0], 3)
    sent(w_ref.at[:, pl.ds(0, nx - 1), 0], 4)
    sent(sums_ref.at[pl.ds(0, nsp - 1)], 5)
    sent(tok_ref.at[pl.ds(0, ntp - 1)], 6)
    sent(w_ref.at[:, :, pl.ds(0, 2)], 7)
    sent(e_ref.at[0, 0, pl.ds(0, nx - 1), 0], 8)
    sent(e_ref.at[0, pl.ds(0, ny - 1), 0, 1], 9)
    sent(e_ref.at[pl.ds(1, 2), 0, pl.ds(0, nx - 1), 0], 11)
    sent(e_ref.at[pl.ds(1, 2), pl.ds(0, ny - 1), 0, 1], 12)
    sent(x_ref.at[pl.ds(0, far - 1)], 10)
    sent(x_ref.at[pl.ds(0, nsp - far)], 14)
    sent(xb_ref, 15)
    for a in range(3):
        sent(e_ref.at[a, pl.ds(0, near_y), :, 0], 18 + a)
        sent(e_ref.at[a, :, pl.ds(0, near_x), 1], 21 + a)
        if ny > 2:
            sent(e_ref.at[a, 0, :, 0], 24 + a)
        if nx > 2:
            sent(e_ref.at[a, :, 0, 1], 27 + a)
    sent(r_ref.at[pl.ds(0, nsp - 1)], 13)


def solution(mesh):
    nsp, ntp = mesh.shape["sp"], mesh.shape["tp"]
    nx = math.isqrt(ntp)
    ny = ntp // nx

    def per_device(
        resid, branch_input, gate_in, conv_taps, rate_weight, input_weight, decay_base,
        decay_extra, out_weight, gain_mix, gain_pre, gain_post, expert_ids, route_weight,
        gate_proj, up_proj, down_proj,
    ):
        chan, positions = branch_input.shape
        toks, width = resid.shape
        blocks = positions // LANES
        cap = 2 * toks // nsp
        vmem = pl.BlockSpec(memory_space=pltpu.VMEM)
        hbm = pl.BlockSpec(memory_space=pltpu.HBM)
        block = (blocks, chan, LANES)
        far = nsp * FAR // 32
        return pl.pallas_call(
            functools.partial(kernel, (nsp, nx, ny)),
            out_shape=jax.ShapeDtypeStruct((toks, width), BF16),
            in_specs=[hbm] * 17,
            out_specs=vmem,
            scratch_shapes=[
                pltpu.VMEM((toks, width), BF16),
                pltpu.VMEM(block, F32),
                pltpu.VMEM(block, F32),
                pltpu.VMEM(block, F32),
                pltpu.VMEM(block, F32),
                pltpu.VMEM(block, F32),
                pltpu.VMEM((chan, LANES), BF16),
                pltpu.VMEM((1, LANES), F32),
                pltpu.VMEM((nsp, 1, LANES), F32),
                pltpu.VMEM(block, BF16),
                pltpu.VMEM((ntp, chan, toks), BF16),
                pltpu.VMEM((ny, nx, 4, chan // 4, width), BF16),
                pltpu.VMEM((3, ny, nx, 2, 16, width), BF16),
                pltpu.VMEM((toks, width), F32),
                pltpu.VMEM((toks, width), BF16),
                pltpu.VMEM((3, nsp * cap, toks), BF16),
                pltpu.VMEM((nsp, cap, width), BF16),
                pltpu.VMEM((nsp, cap, width), BF16),
                pltpu.VMEM((nsp, cap, width), BF16),
                pltpu.VMEM((nsp, cap, ntp * chan), BF16),
                pltpu.VMEM((nsp - far, cap, ntp * chan), BF16),
                pltpu.VMEM(((nsp - far) * cap, width), F32),
                pltpu.VMEM((max(far, nsp - far) * cap, width), BF16),
                pltpu.VMEM((ny // 2, max(far, nsp - far) * cap, nx * 64), BF16),
                pltpu.VMEM((nsp, cap, width), BF16),
                pltpu.VMEM((nsp, cap, width), BF16),
                pltpu.VMEM((toks, width), F32),
                pltpu.VMEM((chan, positions), BF16),
                pltpu.VMEM((chan, positions), BF16),
                pltpu.VMEM(conv_taps.shape, BF16),
                pltpu.VMEM((chan, chan), BF16),
                pltpu.VMEM((chan, chan), BF16),
                pltpu.VMEM((1, chan), F32),
                pltpu.VMEM((blocks, LANES), F32),
                pltpu.VMEM((1, width), F32),
                pltpu.VMEM((1, width), F32),
                pltpu.VMEM((1, width), F32),
                pltpu.VMEM((2, toks), jnp.int32),
                pltpu.VMEM((2, toks), F32),
                pltpu.SemaphoreType.DMA((17,)),
                pltpu.SemaphoreType.DMA((30,)),
                pltpu.SemaphoreType.DMA((30,)),
            ],
            compiler_params=pltpu.CompilerParams(
                collective_id=0, has_side_effects=True, vmem_limit_bytes=67043328
            ),
        )(
            resid, branch_input, gate_in, conv_taps,
            rate_weight.reshape(chan, chan), input_weight.reshape(chan, chan),
            decay_base.reshape(1, chan), decay_extra.reshape(blocks, LANES),
            out_weight.reshape(4, chan // 4, width),
            gain_mix.reshape(1, width), gain_pre.reshape(1, width), gain_post.reshape(1, width),
            expert_ids.T, route_weight.T,
            gate_proj.reshape(2, 16, width), up_proj.reshape(2, 16, width),
            down_proj.reshape(2, 16, width),
        )

    sp_tp = P(("sp", "tp"), None)
    experts = P("sp", "tp", None)
    return jax.shard_map(
        per_device,
        mesh=mesh,
        in_specs=(
            sp_tp, P("tp", "sp"), P("tp", "sp"), P(None, "tp"),
            P("tp", None, None), P("tp", None, None), P("tp"), P("sp"), P("tp", None),
            P(), P(), P(), sp_tp, sp_tp, experts, experts, experts,
        ),
        out_specs=sp_tp,
        check_vma=False,
    )
```

```python
import functools
import math

import jax
import jax.numpy as jnp
from jax import lax
from jax.experimental import pallas as pl
from jax.experimental.pallas import tpu as pltpu
from jax.sharding import PartitionSpec as P

MESH = pl.DeviceIdType.MESH
F32 = jnp.float32
BF16 = jnp.bfloat16

epsilon = 1e-06
gate_power = 8.0
LANES = 128
COLS = 512
GROUP = 4
FAR = 22
FAR_EDGE = "far"
NEAR_EDGE = "near"


def one_minus_exp(y):
    series = F32(1.0 / 362880)
    for k in (40320, 5040, 720, 120, 24, 6, 2, 1):
        series = series * y + F32(1.0 / k)
    return jnp.where(y > -0.5, -y * series, 1.0 - jnp.exp(y))


def softplus(x):
    u = jnp.exp(-jnp.abs(x))
    series = F32(1.0 / 11)
    for k in range(10, 0, -1):
        series = F32(1.0 / k) - series * u
    return jnp.maximum(x, 0.0) + jnp.where(u < 0.125, u * series, jnp.log(1.0 + u))


def gelu(x):
    inner = F32(math.sqrt(2.0 / math.pi)) * (x + F32(0.044715) * (x * x * x))
    return x * (0.5 * (1.0 + jnp.tanh(inner)))


def to_column(row, size):
    lanes = row.shape[1]
    here = lax.broadcasted_iota(jnp.int32, (size, lanes), 0)
    there = lax.broadcasted_iota(jnp.int32, (size, lanes), 1)
    return jnp.sum(jnp.where(here == there, row, 0.0), axis=1, keepdims=True)


def kernel(
    cfg,
    resid_hbm,
    branch_hbm,
    gate_hbm,
    taps_hbm,
    rate_w_hbm,
    input_w_hbm,
    base_hbm,
    extra_hbm,
    outw_hbm,
    gmix_hbm,
    gpre_hbm,
    gpost_hbm,
    ids_hbm,
    rw_hbm,
    gp_hbm,
    up_hbm,
    dp_hbm,
    out_ref,
    resid_ref,
    keep_ref,
    state_ref,
    last_keep,
    last_state,
    act_ref,
    halo_ref,
    sum_ref,
    sums_ref,
    bo_ref,
    tok_ref,
    w_ref,
    e_ref,
    after_ref,
    ffn_ref,
    pick_ref,
    o_ref,
    x_ref,
    on_ref,
    ob_ref,
    xb_ref,
    m_ref,
    xf_ref,
    hid_ref,
    y_ref,
    r_ref,
    moe_ref,
    branch_ref,
    gate_ref,
    taps_ref,
    rate_w_ref,
    input_w_ref,
    base_ref,
    extra_ref,
    gmix_ref,
    gpre_ref,
    gpost_ref,
    ids_ref,
    rw_ref,
    loc_sem,
    send_sem,
    recv_sem,
    out_sem,
):
    nsp, nx, ny = cfg
    ntp = nx * ny
    sp = lax.axis_index("sp")
    tp = lax.axis_index("tp")
    my_x, my_y = lax.rem(tp, nx), lax.div(tp, nx)
    core = lax.rem(sp, 2)
    chan, positions = branch_hbm.shape
    blocks = positions // LANES
    toks, width = resid_hbm.shape
    cap = o_ref.shape[1]
    slots = nsp * cap
    col_steps = width // COLS

    def remote(src, dst, k, to_sp, to_tp):
        return pltpu.make_async_remote_copy(
            src_ref=src, dst_ref=dst, send_sem=send_sem.at[k], recv_sem=recv_sem.at[k],
            device_id=(to_sp, to_tp), device_id_type=MESH,
        )

    def got(ref, k):
        pltpu.make_async_copy(ref, ref, recv_sem.at[k]).wait()

    def sent(ref, k):
        pltpu.make_async_copy(ref, ref, send_sem.at[k]).wait()

    barrier = pltpu.get_barrier_semaphore()

    def greet_sp(k, carry):
        pl.semaphore_signal(
            barrier, inc=1, device_id=(lax.rem(sp + lax.rem(k + nsp // 4 - 1, nsp - 1) + 1, nsp), tp),
            device_id_type=MESH,
        )
        return carry

    def greet_tp(k, carry):
        pl.semaphore_signal(
            barrier, inc=1, device_id=(sp, lax.rem(tp + k, ntp)), device_id_type=MESH
        )
        return carry

    lax.fori_loop(1, nsp, greet_sp, 0)
    lax.fori_loop(1, ntp, greet_tp, 0)

    own = [
        pltpu.make_async_copy(outw_hbm, w_ref.at[my_y, my_x], loc_sem.at[0]),
        pltpu.make_async_copy(gp_hbm, e_ref.at[0, my_y, my_x], loc_sem.at[1]),
        pltpu.make_async_copy(up_hbm, e_ref.at[1, my_y, my_x], loc_sem.at[2]),
        pltpu.make_async_copy(dp_hbm, e_ref.at[2, my_y, my_x], loc_sem.at[3]),
        pltpu.make_async_copy(resid_hbm, resid_ref, loc_sem.at[4]),
    ]
    small = [
        pltpu.make_async_copy(source, target, loc_sem.at[5 + k])
        for k, (source, target) in enumerate((
            (branch_hbm, branch_ref), (taps_hbm, taps_ref), (rate_w_hbm, rate_w_ref),
            (input_w_hbm, input_w_ref), (base_hbm, base_ref), (extra_hbm, extra_ref),
            (gate_hbm, gate_ref), (ids_hbm, ids_ref), (rw_hbm, rw_ref),
            (gmix_hbm, gmix_ref), (gpre_hbm, gpre_ref), (gpost_hbm, gpost_ref),
        ))
    ]
    for copy in small + own:
        copy.start()

    for copy in small[:6]:
        copy.wait()

    taps = taps_ref[...].astype(F32)
    tap_cols = [to_column(taps[j : j + 1, :], chan) for j in range(4)]
    decay_rate = -gate_power * softplus(-to_column(base_ref[...], chan))
    lane = lax.broadcasted_iota(jnp.int32, (chan, LANES), 1)

    def lanes_of(index):
        return pl.ds(pl.multiple_of(index * LANES, LANES), LANES)

    def block_group(first, count, before):
        convs = []
        for g in range(count):
            cur = branch_ref[:, lanes_of(first + g)].astype(F32)
            total = tap_cols[3] * cur
            for back in (1, 2, 3):
                moved = jnp.where(
                    lane < back, pltpu.roll(before, back, 1), pltpu.roll(cur, back, 1)
                )
                total = total + tap_cols[3 - back] * moved
            convs.append(total)
            before = cur
        conv = jnp.concatenate(convs, axis=1)
        high = conv.astype(BF16)
        rest = conv - high.astype(F32)
        mid = rest.astype(BF16)
        low = (rest - mid.astype(F32)).astype(BF16)

        def gate_of(weight_ref):
            w = weight_ref[...]
            total = None
            for piece in (low, mid, high):
                part = lax.dot_general(
                    w, piece, (((0,), (0,)), ((), ())), preferred_element_type=F32
                )
                total = part if total is None else total + part
            return jax.nn.sigmoid(total)

        rate_gate = gate_of(rate_w_ref)
        input_gate = gate_of(input_w_ref)
        for g in range(count):
            at = slice(g * LANES, (g + 1) * LANES)
            extra = extra_ref[pl.ds(first + g, 1), :]
            log_keep = decay_rate * rate_gate[:, at] + extra
            keep = jnp.exp(log_keep)
            state = jnp.sqrt(one_minus_exp(2.0 * log_keep)) * input_gate[:, at] * convs[g]
            step = 1
            while step < LANES:
                inside = lane >= step
                keep_back = jnp.where(inside, pltpu.roll(keep, step, 1), 1.0)
                state_back = jnp.where(inside, pltpu.roll(state, step, 1), 0.0)
                state = keep * state_back + state
                keep = keep * keep_back
                step *= 2
            keep_ref[first + g] = keep
            state_ref[first + g] = state
            last_keep[first + g] = jnp.broadcast_to(keep[:, LANES - 1 :], (chan, LANES))
            last_state[first + g] = jnp.broadcast_to(state[:, LANES - 1 :], (chan, LANES))

    group = min(GROUP, blocks)

    def later_group(index, carry):
        first = index * group
        block_group(first, group, branch_ref[:, lanes_of(first - 1)].astype(F32))
        return carry


    for copy in small[6:]:
        copy.wait()

    ids = ids_ref[...]
    expert = lax.broadcasted_iota(jnp.int32, (nsp, toks), 0)
    named = [expert == ids[k : k + 1, :] for k in range(2)]
    counts = (named[0] | named[1]).astype(F32)
    token_a = lax.broadcasted_iota(jnp.int32, (toks, toks), 0)
    token_b = lax.broadcasted_iota(jnp.int32, (toks, toks), 1)
    earlier = jnp.dot(
        counts.astype(BF16), (token_a < token_b).astype(F32).astype(BF16),
        preferred_element_type=F32,
    )
    slot_at = [
        jnp.sum(
            jnp.where(named[k], earlier + (expert * cap).astype(F32), 0.0), axis=0, keepdims=True
        ).astype(jnp.int32)
        for k in range(2)
    ]
    slot = lax.broadcasted_iota(jnp.int32, (slots, toks), 0)
    chosen = [slot == slot_at[k] for k in range(2)]
    pick_ref[0] = (chosen[0] | chosen[1]).astype(F32).astype(BF16)
    weight = jnp.where(chosen[0], rw_ref[0:1, :], 0.0) + jnp.where(chosen[1], rw_ref[1:2, :], 0.0)
    weight_high = weight.astype(BF16)
    pick_ref[1] = weight_high
    pick_ref[2] = (weight - weight_high.astype(F32)).astype(BF16)

    own[4].wait()

    def cols_of(index):
        return pl.ds(pl.multiple_of(index * COLS, COLS), COLS)

    def spread(rows_ref, slots_ref):
        def some(index, carry):
            cols = cols_of(index)
            slots_ref[:, :, cols] = (
                jnp.dot(pick_ref[0], rows_ref[:, cols], preferred_element_type=F32)
                .astype(BF16)
                .reshape(nsp, cap, COLS)
            )
            return carry

        lax.fori_loop(0, col_steps, some, 0)

    spread(resid_ref, o_ref)

    far = nsp * FAR // 32

    def peer(k):
        away = lax.div(k + 1, 2)
        return lax.rem(lax.rem(k, 2) * away + (1 - lax.rem(k, 2)) * (nsp - away) + sp, nsp)

    if (far // 2) % 4 == 2:
        reach = nsp - far // 2 + lax.rem(lax.div(sp, 2), 2) * far
        ahead, behind = lax.rem(sp + nsp - reach + nsp, nsp), lax.rem(sp + reach, nsp)
        from_far, from_near = ahead, behind
    else:
        ahead, behind = peer(far - 1), peer(far)
        from_far, from_near = behind, ahead

    def send_block(source, target, sem, k, place):
        to = ahead if k is FAR_EDGE else behind if k is NEAR_EDGE else peer(k)
        remote(source.at[to], target.at[place], sem, to, tp).start()

    def send_blocks(source, target, sem, begin, end, offset=0):
        def step(k, carry):
            send_block(source, target, sem, k, k + 2 * lax.rem(k, 2) - 1 - offset)
            return carry

        lax.fori_loop(begin, end, step, 0)

    first_batch = min(far + 2, nsp - 1)

    early_groups = min(2, blocks // group)
    lax.fori_loop(early_groups + 1, blocks // group, later_group, 0)

    pl.semaphore_wait(barrier, nsp - 1 + ntp - 1)
    remote(
        branch_ref.at[:, pl.ds(positions - LANES, LANES)], halo_ref, 0, lax.rem(sp + 1, nsp), tp
    ).start()

    send_block(o_ref, x_ref, 14, FAR_EDGE, far)
    send_blocks(o_ref, x_ref, 14, far + 1, first_batch)

    own[0].wait()
    half_a, half_b = 2 * core, 2 * core + 1

    def tp_at(y, x):
        return lax.rem(y, ny) * nx + lax.rem(x, nx)

    for k in range(1, nx):
        ref = w_ref.at[my_y, my_x, half_a]
        remote(ref, ref, 1, sp, tp_at(my_y, my_x + k)).start()
    for k in range(1, ny):
        ref = w_ref.at[my_y, my_x, half_b]
        remote(ref, ref, 2, sp, tp_at(my_y + k, my_x)).start()

    for copy in own[1:4]:
        copy.wait()
    for k in range(1, nx):
        ref = e_ref.at[0, my_y, my_x, 0]
        remote(ref, ref, 8, sp, tp_at(my_y, my_x + k)).start()
    for k in range(1, ny):
        ref = e_ref.at[0, my_y, my_x, 1]
        remote(ref, ref, 9, sp, tp_at(my_y + k, my_x)).start()

    lax.fori_loop(1, min(early_groups + 1, blocks // group), later_group, 0)
    block_group(1, group - 1, branch_ref[:, lanes_of(0)].astype(F32))
    got(halo_ref, 0)
    block_group(0, 1, jnp.where(sp == 0, 0.0, halo_ref[...].astype(F32)))

    def chain(index, carry):
        keep, state = carry
        block_keep, block_state = last_keep[index], last_state[index]
        last_keep[index] = keep
        last_state[index] = state
        return (block_keep * keep, block_keep * state + block_state)

    all_keep, all_state = lax.fori_loop(
        0, blocks, chain, (jnp.ones((chan, LANES), F32), jnp.zeros((chan, LANES), F32))
    )
    row = lax.broadcasted_iota(jnp.int32, (chan, LANES), 0)
    summary = jnp.where(lane == row, all_keep, 0.0) + jnp.where(
        lane == row + chan, all_state, 0.0
    )
    sum_ref[...] = jnp.sum(summary, axis=0, keepdims=True)
    sums_ref[sp] = sum_ref[...]

    def send_summary(k, carry):
        remote(sum_ref, sums_ref.at[sp], 5, lax.rem(sp + k, nsp), tp).start()
        return carry

    lax.fori_loop(1, nsp, send_summary, 0)
    send_blocks(o_ref, x_ref, 14, first_batch, nsp - 1)
    send_block(o_ref, x_ref, 14, nsp - 1, nsp - 1)

    got(w_ref.at[0, pl.ds(0, nx - 1), 0], 1)
    for k in range(1, ny):
        ref = w_ref.at[my_y, :, half_a]
        remote(ref, ref, 3, sp, tp_at(my_y + k, my_x)).start()
    got(w_ref.at[pl.ds(0, ny - 1), 0, 0], 2)
    for k in range(1, nx):
        ref = w_ref.at[:, my_x, half_b]
        remote(ref, ref, 4, sp, tp_at(my_y, my_x + k)).start()

    def activate(index, carry):
        act_ref[index] = gelu(gate_ref[:, lanes_of(index)].astype(F32))
        return carry

    lax.fori_loop(0, blocks, activate, 0)

    got(sums_ref.at[pl.ds(0, nsp - 1)], 5)

    def fold(index, carry):
        line = sums_ref[index]
        keep = jnp.where(index < sp, to_column(line, chan), 1.0)
        moved = jnp.where(
            index < sp,
            jnp.sum(jnp.where(lane == row + chan, line, 0.0), axis=1, keepdims=True),
            0.0,
        )
        return keep * carry + moved

    entering = lax.fori_loop(0, nsp, fold, jnp.zeros((chan, 1), F32), unroll=True)

    def finish(index, carry):
        begin = last_state[index] + last_keep[index] * entering
        hidden = state_ref[index] + keep_ref[index] * begin
        bo_ref[index] = (hidden * act_ref[index]).astype(BF16)
        return carry

    lax.fori_loop(0, blocks, finish, 0)

    def send_tokens(k, carry):
        to = lax.rem(tp + k, ntp)
        remote(bo_ref.at[to], tok_ref.at[tp], 6, sp, to).start()
        return carry

    lax.fori_loop(1, ntp, send_tokens, 0)
    tok_ref[tp] = bo_ref[tp]

    for k in range(1, nx):
        ref = e_ref.at[pl.ds(1, 2), my_y, my_x, 0]
        remote(ref, ref, 11, sp, tp_at(my_y, my_x + k)).start()
    for k in range(1, ny):
        ref = e_ref.at[pl.ds(1, 2), my_y, my_x, 1]
        remote(ref, ref, 12, sp, tp_at(my_y + k, my_x)).start()

    def second_leg(a):
        for k in sorted({1, ny - 1}):
            ref = e_ref.at[a, my_y, :, 0]
            remote(ref, ref, 18 + a, sp, tp_at(my_y + k, my_x)).start()
        for k in sorted({1, nx - 1}):
            ref = e_ref.at[a, :, my_x, 1]
            remote(ref, ref, 21 + a, sp, tp_at(my_y, my_x + k)).start()

    got(e_ref.at[0, 0, pl.ds(0, nx - 1), 0], 8)
    got(e_ref.at[0, pl.ds(0, ny - 1), 0, 1], 9)
    second_leg(0)

    got(w_ref.at[pl.ds(0, ny - 1), :, 0], 3)
    got(w_ref.at[:, pl.ds(0, nx - 1), 0], 4)
    ref = w_ref.at[:, :, pl.ds(2 * core, 2)]
    remote(ref, ref, 7, sp + 1 - 2 * core, tp).start()

    got(tok_ref.at[pl.ds(0, ntp - 1)], 6)
    ob_ref[...] = (
        lax.dot_general(
            pick_ref[0], tok_ref[...].reshape(ntp * chan, toks), (((1,), (1,)), ((), ())),
            preferred_element_type=F32,
        )
        .astype(BF16)
        .reshape(nsp, cap, ntp * chan)
    )
    send_block(ob_ref, xb_ref, 15, FAR_EDGE, 0)
    send_blocks(ob_ref, xb_ref, 15, far + 1, nsp - 1, far)
    send_block(ob_ref, xb_ref, 15, nsp - 1, nsp - 1 - far)

    got(w_ref.at[:, :, pl.ds(0, 2)], 7)

    def scale(values):
        return lax.rsqrt(jnp.mean(values * values, axis=-1, keepdims=True) + epsilon)

    def rows_of(index):
        return pl.ds(pl.multiple_of(index * 16, 16), 16)

    def projection(cols):
        return w_ref[:, :, :, :, cols].reshape(ntp * chan, COLS)

    def mix(index, carry):
        cols = cols_of(index)
        rows = tok_ref[...].reshape(ntp * chan, toks)
        moe_ref[:, cols] = lax.dot_general(
            rows, projection(cols), (((0,), (0,)), ((), ())), preferred_element_type=F32
        )
        return carry

    lax.fori_loop(0, col_steps, mix, 0)

    def norms(index, carry):
        rows = rows_of(index)
        mixed = moe_ref[rows, :]
        after = resid_ref[rows, :].astype(F32) + mixed * scale(mixed) * gmix_ref[...]
        after_ref[rows, :] = after
        ffn_ref[rows, :] = (after * scale(after) * gpre_ref[...]).astype(BF16)
        return carry

    lax.fori_loop(0, toks // 16, norms, 0, unroll=2)

    spread(ffn_ref, on_ref)
    send_blocks(on_ref, x_ref, 10, 1, far - 1)
    send_block(on_ref, x_ref, 10, NEAR_EDGE, far - 1)
    x_ref[0] = on_ref[sp]

    got(e_ref.at[pl.ds(1, 2), 0, pl.ds(0, nx - 1), 0], 11)
    got(e_ref.at[pl.ds(1, 2), pl.ds(0, ny - 1), 0, 1], 12)
    second_leg(1)
    second_leg(2)
    near_y, near_x = min(2, ny - 1), min(2, nx - 1)
    low, high = pl.ds(0, width // 2), pl.ds(width // 2, width // 2)
    for a in range(3):
        got(e_ref.at[a, pl.ds(0, near_y), :, 0], 18 + a)
        if ny > 2:
            before, after = lax.rem(my_y + ny - 1, ny), lax.rem(my_y + 1, ny)
            ref = e_ref.at[a, before, :, 0, :, low]
            remote(ref, ref, 24 + a, sp, tp_at(after, my_x)).start()
            ref = e_ref.at[a, after, :, 0, :, high]
            remote(ref, ref, 24 + a, sp, tp_at(before, my_x)).start()
        got(e_ref.at[a, :, pl.ds(0, near_x), 1], 21 + a)
        if nx > 2:
            before, after = lax.rem(my_x + nx - 1, nx), lax.rem(my_x + 1, nx)
            ref = e_ref.at[a, :, before, 1, :, low]
            remote(ref, ref, 27 + a, sp, tp_at(my_y, after)).start()
            ref = e_ref.at[a, :, after, 1, :, high]
            remote(ref, ref, 27 + a, sp, tp_at(my_y, before)).start()

    def whole_weights(a):
        if ny > 2:
            got(e_ref.at[a, 0, :, 0], 24 + a)
        if nx > 2:
            got(e_ref.at[a, :, 0, 1], 27 + a)

    per_y = nx * 32
    nt = (((1,), (1,)), ((), ()))
    sources = max(16 // cap, 1)

    def rows_at(index):
        count = sources * cap
        return pl.ds(pl.multiple_of(index * count, count), count)

    def blocks_at(base, index):
        return x_ref[pl.ds(base + index * sources, sources)].reshape(sources * cap, width)

    def serve(base, end, first):
        rows = (end - base) * cap
        if first:
            whole_weights(0)
            whole_weights(1)

        def expert_in(index, carry):
            ys = pl.ds(index * 2, 2)
            gate_rows = e_ref[0, ys].reshape(2 * per_y, width)
            up_rows = e_ref[1, ys].reshape(2 * per_y, width)
            inputs = xf_ref[0:rows, :]
            gate_vals = lax.dot_general(inputs, gate_rows, nt, preferred_element_type=F32)
            up_vals = lax.dot_general(inputs, up_rows, nt, preferred_element_type=F32)
            hid_ref[index, 0:rows, :] = (
                gate_vals * jax.nn.sigmoid(gate_vals) * up_vals
            ).astype(BF16)
            return carry

        lax.fori_loop(0, ny // 2, expert_in, 0)

        if first:
            whole_weights(2)

        def expert_out(index, carry):
            cols = cols_of(index)
            total = None
            for pair in range(ny // 2):
                down = e_ref[2, 2 * pair : 2 * pair + 2, :, :, :, cols].reshape(2 * per_y, COLS)
                product = jnp.dot(hid_ref[pair, 0:rows, :], down, preferred_element_type=F32)
                total = product if total is None else total + product
            y_ref[base:end, :, cols] = total.astype(BF16).reshape(end - base, cap, COLS)
            return carry

        lax.fori_loop(0, col_steps, expert_out, 0)

        def give_back(k, carry):
            remote(y_ref.at[k], r_ref.at[sp], 13, peer(k), tp).start()
            return carry

        if first:
            lax.fori_loop(far + 1, nsp, give_back, 0)
            remote(y_ref.at[far], r_ref.at[sp], 13, from_far, tp).start()
        else:
            lax.fori_loop(1, far - 1, give_back, 0)
            remote(y_ref.at[far - 1], r_ref.at[sp], 13, from_near, tp).start()

    got(x_ref.at[pl.ds(0, nsp - far)], 14)
    got(xb_ref, 15)

    def mix_arrived(index, carry):
        cols = cols_of(index)
        m_ref[:, cols] = jnp.dot(
            xb_ref[...].reshape((nsp - far) * cap, ntp * chan), projection(cols),
            preferred_element_type=F32,
        )
        return carry

    lax.fori_loop(0, col_steps, mix_arrived, 0)

    def norm_arrived(index, carry):
        rows = rows_at(index)
        mixed = m_ref[rows, :]
        after = (
            blocks_at(far, index).astype(F32) + mixed * scale(mixed) * gmix_ref[...]
        )
        xf_ref[rows, :] = (after * scale(after) * gpre_ref[...]).astype(BF16)
        return carry

    lax.fori_loop(0, (nsp - far) // sources, norm_arrived, 0, unroll=2)
    serve(far, nsp, True)

    got(x_ref.at[pl.ds(0, far - 1)], 10)

    def take_arrived(index, carry):
        xf_ref[rows_at(index), :] = blocks_at(0, index)
        return carry

    lax.fori_loop(0, far // sources, take_arrived, 0)
    serve(0, far, False)
    r_ref[sp] = y_ref[0]
    got(r_ref.at[pl.ds(0, nsp - 1)], 13)

    def combine(index, carry):
        cols = cols_of(index)
        rows = r_ref[:, :, cols].reshape(slots, COLS)
        tn = (((0,), (0,)), ((), ()))
        moe_ref[:, cols] = lax.dot_general(
            pick_ref[2], rows, tn, preferred_element_type=F32
        ) + lax.dot_general(pick_ref[1], rows, tn, preferred_element_type=F32)
        return carry

    lax.fori_loop(0, col_steps, combine, 0)

    def put_out(index):
        rows = rows_of(index)
        pltpu.make_async_copy(ffn_ref.at[rows, :], out_ref.at[rows, :], out_sem).start()

    def finalize(index, carry):
        rows = rows_of(index)
        moe = moe_ref[rows, :]
        ffn_ref[rows, :] = (after_ref[rows, :] + moe * scale(moe) * gpost_ref[...]).astype(BF16)

        @pl.when(index > 0)
        def _():
            put_out(index - 1)

        return carry

    lax.fori_loop(0, toks // 16, finalize, 0, unroll=2)

    put_out(toks // 16 - 1)

    sent(halo_ref, 0)
    sent(w_ref.at[0, pl.ds(0, nx - 1), 0], 1)
    sent(w_ref.at[pl.ds(0, ny - 1), 0, 0], 2)
    sent(w_ref.at[pl.ds(0, ny - 1), :, 0], 3)
    sent(w_ref.at[:, pl.ds(0, nx - 1), 0], 4)
    sent(sums_ref.at[pl.ds(0, nsp - 1)], 5)
    sent(tok_ref.at[pl.ds(0, ntp - 1)], 6)
    sent(w_ref.at[:, :, pl.ds(0, 2)], 7)
    sent(e_ref.at[0, 0, pl.ds(0, nx - 1), 0], 8)
    sent(e_ref.at[0, pl.ds(0, ny - 1), 0, 1], 9)
    sent(e_ref.at[pl.ds(1, 2), 0, pl.ds(0, nx - 1), 0], 11)
    sent(e_ref.at[pl.ds(1, 2), pl.ds(0, ny - 1), 0, 1], 12)
    sent(x_ref.at[pl.ds(0, far - 1)], 10)
    sent(x_ref.at[pl.ds(0, nsp - far)], 14)
    sent(xb_ref, 15)
    for a in range(3):
        sent(e_ref.at[a, pl.ds(0, near_y), :, 0], 18 + a)
        sent(e_ref.at[a, :, pl.ds(0, near_x), 1], 21 + a)
        if ny > 2:
            sent(e_ref.at[a, 0, :, 0], 24 + a)
        if nx > 2:
            sent(e_ref.at[a, :, 0, 1], 27 + a)
    sent(r_ref.at[pl.ds(0, nsp - 1)], 13)
    pltpu.make_async_copy(ffn_ref, out_ref, out_sem).wait()


def solution(mesh):
    nsp, ntp = mesh.shape["sp"], mesh.shape["tp"]
    nx = math.isqrt(ntp)
    ny = ntp // nx

    def per_device(
        resid, branch_input, gate_in, conv_taps, rate_weight, input_weight, decay_base,
        decay_extra, out_weight, gain_mix, gain_pre, gain_post, expert_ids, route_weight,
        gate_proj, up_proj, down_proj,
    ):
        chan, positions = branch_input.shape
        toks, width = resid.shape
        blocks = positions // LANES
        cap = 2 * toks // nsp
        hbm = pl.BlockSpec(memory_space=pltpu.HBM)
        block = (blocks, chan, LANES)
        far = nsp * FAR // 32
        return pl.pallas_call(
            functools.partial(kernel, (nsp, nx, ny)),
            out_shape=jax.ShapeDtypeStruct((toks, width), BF16),
            in_specs=[hbm] * 17,
            out_specs=hbm,
            scratch_shapes=[
                pltpu.VMEM((toks, width), BF16),
                pltpu.VMEM(block, F32),
                pltpu.VMEM(block, F32),
                pltpu.VMEM(block, F32),
                pltpu.VMEM(block, F32),
                pltpu.VMEM(block, F32),
                pltpu.VMEM((chan, LANES), BF16),
                pltpu.VMEM((1, LANES), F32),
                pltpu.VMEM((nsp, 1, LANES), F32),
                pltpu.VMEM(block, BF16),
                pltpu.VMEM((ntp, chan, toks), BF16),
                pltpu.VMEM((ny, nx, 4, chan // 4, width), BF16),
                pltpu.VMEM((3, ny, nx, 2, 16, width), BF16),
                pltpu.VMEM((toks, width), F32),
                pltpu.VMEM((toks, width), BF16),
                pltpu.VMEM((3, nsp * cap, toks), BF16),
                pltpu.VMEM((nsp, cap, width), BF16),
                pltpu.VMEM((nsp, cap, width), BF16),
                pltpu.VMEM((nsp, cap, width), BF16),
                pltpu.VMEM((nsp, cap, ntp * chan), BF16),
                pltpu.VMEM((nsp - far, cap, ntp * chan), BF16),
                pltpu.VMEM(((nsp - far) * cap, width), F32),
                pltpu.VMEM((max(far, nsp - far) * cap, width), BF16),
                pltpu.VMEM((ny // 2, max(far, nsp - far) * cap, nx * 64), BF16),
                pltpu.VMEM((nsp, cap, width), BF16),
                pltpu.VMEM((nsp, cap, width), BF16),
                pltpu.VMEM((toks, width), F32),
                pltpu.VMEM((chan, positions), BF16),
                pltpu.VMEM((chan, positions), BF16),
                pltpu.VMEM(conv_taps.shape, BF16),
                pltpu.VMEM((chan, chan), BF16),
                pltpu.VMEM((chan, chan), BF16),
                pltpu.VMEM((1, chan), F32),
                pltpu.VMEM((blocks, LANES), F32),
                pltpu.VMEM((1, width), F32),
                pltpu.VMEM((1, width), F32),
                pltpu.VMEM((1, width), F32),
                pltpu.VMEM((2, toks), jnp.int32),
                pltpu.VMEM((2, toks), F32),
                pltpu.SemaphoreType.DMA((17,)),
                pltpu.SemaphoreType.DMA((30,)),
                pltpu.SemaphoreType.DMA((30,)),
                pltpu.SemaphoreType.DMA,
            ],
            compiler_params=pltpu.CompilerParams(
                collective_id=0, has_side_effects=True, vmem_limit_bytes=67043328
            ),
        )(
            resid, branch_input, gate_in, conv_taps,
            rate_weight.reshape(chan, chan), input_weight.reshape(chan, chan),
            decay_base.reshape(1, chan), decay_extra.reshape(blocks, LANES),
            out_weight.reshape(4, chan // 4, width),
            gain_mix.reshape(1, width), gain_pre.reshape(1, width), gain_post.reshape(1, width),
            expert_ids.T, route_weight.T,
            gate_proj.reshape(2, 16, width), up_proj.reshape(2, 16, width),
            down_proj.reshape(2, 16, width),
        )

    sp_tp = P(("sp", "tp"), None)
    experts = P("sp", "tp", None)
    return jax.shard_map(
        per_device,
        mesh=mesh,
        in_specs=(
            sp_tp, P("tp", "sp"), P("tp", "sp"), P(None, "tp"),
            P("tp", None, None), P("tp", None, None), P("tp"), P("sp"), P("tp", None),
            P(), P(), P(), sp_tp, sp_tp, experts, experts, experts,
        ),
        out_specs=sp_tp,
        check_vma=False,
    )
```
